32 devices in a mesh: dp: 4 (over y, x), kv: 4 (over z), tp: 2 (over core).
Axes of the slice: x: 2, y: 2, z: 4, core: 2. Of those that a mesh axis runs over, the one named last changes fastest.
Arguments:
- pieces: bfloat16 [4096, 8, 2048], P(('kv', 'tp'), 'dp'), parts along dimension 1, may hold values from -6 to 6
- new_tokens: bfloat16 [256, 2048], P(('dp', 'kv', 'tp')), parts along dimension 0, may hold values from -6 to 6
- w_query: bfloat16 [2048, 1024], P(None, 'tp'), may hold values from -0.125 to 0.125
- w_key: bfloat16 [2048, 1024], P(None, 'tp'), may hold values from -0.125 to 0.125
- w_value: bfloat16 [2048, 2048], P(None, 'tp'), may hold values from -0.125 to 0.125
- w_decay: bfloat16 [2048, 1024], P(None, 'tp'), may hold values from -0.125 to 0.125
- decay_bias: float32 [1024], replicated, may hold values from 0 to 9
- norm_gain: float32 [2048], replicated, may hold values from 0.1 to 1.9
- head_gain: float32 [2048], replicated, may hold values from 0.1 to 1.9
- w_out: bfloat16 [2048, 2048], replicated, may hold values from -0.125 to 0.125
- prompt_state: float32 [8, 8, 128, 256], P('dp', 'tp', 'kv'), parts along dimension 0, may hold values from -8 to 8
- decode_state: float32 [256, 8, 128, 256], P(('dp', 'kv'), 'tp'), parts along dimension 0, may hold values from -8 to 8
Outputs:
- mixed_piece: bfloat16 [4096, 8, 2048], P(('kv', 'tp'), 'dp'), parts along dimension 1
- mixed_decode: bfloat16 [256, 2048], P(('dp', 'kv', 'tp')), parts along dimension 0
- prompt_state_out: float32 [8, 8, 128, 256], P('dp', 'tp', 'kv'), parts along dimension 0
- decode_state_out: float32 [256, 8, 128, 256], P(('dp', 'kv'), 'tp'), parts along dimension 0
The draws below stay inside these ranges and needn't reach their ends.
There are 4 independent parts, one for each index of `dp`. The reference program is written for one: setup_inputs(seed, part) draws one part's arguments, and reference() takes and returns one part's arrays. A program takes and returns all parts, laid end to end along the dimension named above; an argument that names none is the same for every part. Nothing has to cross between parts.
All inputs are finite; a program needn't handle non-finite values.
Results may differ from the reference program's by a relative error of at most 0.014.
Values may be sent and summed in bfloat16 or wider, within the bound.
A program may use at most 192 MiB of HBM per device.

```python
import jax
import jax.numpy as jnp
from jax import lax

D = 2048
HEADS = 8
DK = 128
DV = 256
BLOCK = 64
PROMPTS = 2
PIECE = 4096
DEC = 64


def block_scale(rng, extent, cuts, smallest, high):
    def one(axis_at, blocks):
        draws = jax.random.uniform(jax.random.fold_in(jax.random.fold_in(rng, 6), axis_at), (blocks,), jnp.float32, smallest / len(cuts), high / len(cuts))
        return jnp.repeat(jnp.exp(draws), extent[axis_at] // blocks).reshape((-1,) + (1,) * (len(extent) - axis_at - 1))

    level = one(*cuts[0])
    for cut in cuts[1:]:
        level = level * one(*cut)
    return level


def centred(rng, dims, spread, bound, cuts=(), held_as=jnp.bfloat16):
    values = spread * jax.random.normal(rng, dims, jnp.float32)
    if cuts:
        values = values * block_scale(rng, dims, cuts, -0.22, 0.18)
    return jnp.clip(values, -bound, bound).astype(held_as)


def setup_inputs(seed: int = 0, part: int = 0) -> dict:
    key_of = jax.random.split(jax.random.key(seed), 13)
    own_keys = jax.random.split(jax.random.fold_in(key_of[12], part), 13)
    return {
        "pieces": centred(own_keys[0], (PIECE, PROMPTS, D), 1.0, 6.0, ((0, 8),)),
        "new_tokens": centred(own_keys[1], (DEC, D), 1.0, 6.0, ((0, 8),)),
        "w_query": centred(key_of[2], (D, HEADS * DK), D ** -0.5, 0.125, ((1, 2),)),
        "w_key": centred(key_of[3], (D, HEADS * DK), D ** -0.5, 0.125, ((1, 2),)),
        "w_value": centred(key_of[4], (D, HEADS * DV), D ** -0.5, 0.125, ((1, 2),)),
        "w_decay": centred(key_of[5], (D, HEADS * DK), D ** -0.5, 0.125, ((1, 2),)),
        "decay_bias": jnp.clip(jax.random.uniform(key_of[6], (HEADS * DK,), jnp.float32, 0.0, 9.0), 0.0, 9.0),
        "norm_gain": jnp.clip(1.0 + 0.18 * jax.random.normal(key_of[7], (D,), jnp.float32), 0.1, 1.9),
        "head_gain": jnp.clip(1.0 + 0.18 * jax.random.normal(key_of[8], (HEADS * DV,), jnp.float32), 0.1, 1.9),
        "w_out": centred(key_of[9], (HEADS * DV, D), (HEADS * DV) ** -0.5, 0.125),
        "prompt_state": centred(own_keys[10], (PROMPTS, HEADS, DK, DV), 2.0, 8.0, ((1, 2), (2, 4)), jnp.float32),
        "decode_state": centred(own_keys[11], (DEC, HEADS, DK, DV), 2.0, 8.0, ((0, 4), (1, 2)), jnp.float32),
    }


highest = lax.Precision.HIGHEST
norm_eps = 0.1
decay_tau = 16.0
part_limit = 16

def rms_rows(row_block, gain):
    wide = row_block.astype(jnp.float32)
    factor = lax.rsqrt(lax.optimization_barrier(jnp.mean(wide * wide, axis=-1, keepdims=True)) + norm_eps)
    return (wide * factor * gain).astype(jnp.bfloat16)

def head_norm(outputs, gain):
    factor = lax.rsqrt(lax.optimization_barrier(jnp.mean(outputs * outputs, axis=-1, keepdims=True)) + norm_eps)
    flat = (outputs * factor).reshape(outputs.shape[:-2] + (-1,))
    return (flat * gain).astype(jnp.bfloat16)

def project_roles(row_block, w_query, w_key, w_value, w_decay, decay_bias):
    lead = row_block.shape[:-1]
    queries = (jnp.dot(row_block, w_query, preferred_element_type=jnp.float32) * DK ** (-0.5)).astype(jnp.bfloat16)
    keys_new = jnp.dot(row_block, w_key, preferred_element_type=jnp.float32).astype(jnp.bfloat16)
    values_new = jnp.dot(row_block, w_value, preferred_element_type=jnp.float32).astype(jnp.bfloat16)
    decays = jax.nn.log_sigmoid(jnp.dot(row_block, w_decay, preferred_element_type=jnp.float32) + decay_bias) / decay_tau
    return (queries.reshape(lead + (HEADS, DK)), keys_new.reshape(lead + (HEADS, DK)), values_new.reshape(lead + (HEADS, DV)), decays.reshape(lead + (HEADS, DK)))

def block_terms(q_blk, k_blk, v_blk, g_blk):
    block_len = q_blk.shape[0]
    part_len = min(part_limit, block_len)
    part_count = block_len // part_len
    within = jnp.cumsum(g_blk, axis=0)
    part_ends = within[part_len - 1::part_len]
    anchor = jnp.concatenate([jnp.zeros_like(part_ends[:1]), part_ends[:-1]], axis=0)
    q_wide = q_blk.astype(jnp.float32)
    k_wide = k_blk.astype(jnp.float32)
    q_parts = q_wide.reshape((part_count, part_len) + q_blk.shape[1:])
    w_parts = within.reshape((part_count, part_len) + within.shape[1:])
    near_query = (q_parts * jnp.exp(w_parts - anchor[:, None])).astype(jnp.bfloat16)
    near_key = (k_wide[None] * jnp.exp(anchor[:, None] - within[None])).astype(jnp.bfloat16)
    scores = jnp.einsum('itbhk,isbhk->ibhts', near_query, near_key, preferred_element_type=jnp.float32)
    row_pos = jnp.arange(part_count)[:, None] * part_len + jnp.arange(part_len)[None]
    keep = row_pos[:, :, None] >= jnp.arange(block_len)[None, None]
    weights = jnp.where(keep[:, None, None], scores, 0.0).astype(jnp.bfloat16)
    in_block = jnp.einsum('ibhts,sbhv->itbhv', weights, v_blk, preferred_element_type=jnp.float32)
    in_block = in_block.reshape((block_len,) + in_block.shape[2:])
    block_total = within[-1]
    start_query = (q_wide * jnp.exp(within)).astype(jnp.bfloat16)
    end_key = (k_wide * jnp.exp(block_total[None] - within)).astype(jnp.bfloat16)
    added = jnp.einsum('sbhk,sbhv->bhkv', end_key, v_blk, preferred_element_type=jnp.float32)
    return (in_block, start_query, block_total, added)

def block_attention(query_all, key_all, value_all, decay_all, start_states):
    seq_len = query_all.shape[0]
    block_count = seq_len // BLOCK

    def to_blocks(tensor):
        return tensor.reshape((block_count, BLOCK) + tensor.shape[1:])

    def advance(states, inputs):
        in_block, start_query, block_total, added = block_terms(*inputs)
        from_state = jnp.einsum('tbhk,bhkv->tbhv', start_query.astype(jnp.float32), states, precision=highest)
        carried = jnp.exp(block_total)[..., None] * states + added
        return (carried, from_state + in_block)
    final_states, outputs = lax.scan(advance, start_states, (to_blocks(query_all), to_blocks(key_all), to_blocks(value_all), to_blocks(decay_all)))
    return (outputs.reshape((seq_len,) + outputs.shape[2:]), final_states)

def single_token(query, key_new, value_new, decay, states):
    query = query.astype(jnp.float32)
    key_new = key_new.astype(jnp.float32)
    value_new = value_new.astype(jnp.float32)
    from_state = jnp.einsum('bhk,bhkv->bhv', query * jnp.exp(decay), states, precision=highest)
    token_score = lax.optimization_barrier(jnp.sum(query * key_new, axis=-1, keepdims=True))
    outputs = from_state + token_score * value_new
    carried = jnp.exp(decay)[..., None] * states + key_new[..., None] * value_new[..., None, :]
    return (outputs, carried)

def reference(pieces, new_tokens, w_query, w_key, w_value, w_decay, decay_bias, norm_gain, head_gain, w_out, prompt_state, decode_state):
    query_p, key_p, value_p, decay_p = project_roles(rms_rows(pieces, norm_gain), w_query, w_key, w_value, w_decay, decay_bias)
    piece_att, prompt_out = block_attention(query_p, key_p, value_p, decay_p, prompt_state)
    query_d, key_d, value_d, decay_d = project_roles(rms_rows(new_tokens, norm_gain), w_query, w_key, w_value, w_decay, decay_bias)
    decode_att, decode_out = single_token(query_d, key_d, value_d, decay_d, decode_state)
    mixed_piece = jnp.dot(head_norm(piece_att, head_gain), w_out, preferred_element_type=jnp.float32).astype(jnp.bfloat16)
    mixed_decode = jnp.dot(head_norm(decode_att, head_gain), w_out, preferred_element_type=jnp.float32).astype(jnp.bfloat16)
    return (mixed_piece, mixed_decode, prompt_out, decode_out)
```

```python
import functools

import jax
import jax.numpy as jnp
import numpy as np
from jax import lax
from jax.experimental import pallas as pl
from jax.experimental.pallas import tpu as pltpu
from jax.sharding import PartitionSpec as P

DK = 128
DV = 256
STEP = 64
PART = 16

norm_eps = 0.1
decay_tau = 16.0
f32, bf16 = jnp.float32, jnp.bfloat16
MESH = pl.DeviceIdType.MESH
PAD = 16


def dot(a, b):
    return jnp.dot(a, b, preferred_element_type=f32)


def dot_nt(a, b):
    return lax.dot_general(a, b, (((1,), (1,)), ((), ())), preferred_element_type=f32)


def dot_tn(a, b):
    return lax.dot_general(a, b, (((0,), (0,)), ((), ())), preferred_element_type=f32)


def sum_matrices(prompts):
    n = STEP * prompts
    r, c = np.arange(n)[:, None], np.arange(n)[None]
    same = (r % prompts) == (c % prompts)

    def from_anchor(edge):
        return (same & (c >= edge) & (c <= r)) * 1.0 - (same & (c < edge) & (c > r)) * 1.0

    b = (same & (c <= r)) * 1.0
    rest = (same & (c > r)) * 1.0
    whole = ((np.arange(16)[:, None] == (c % prompts))) * 1.0
    d0 = from_anchor(PART * prompts)[: n // 2]
    d1 = from_anchor(3 * PART * prompts)
    for_keys = np.concatenate([rest, whole], axis=0)
    near = np.concatenate([b, d0, d1], axis=0)
    return np.concatenate([for_keys] * 2, axis=1), np.concatenate([near] * 2, axis=1)


def normed(rows, gain):
    wide = rows.astype(f32)
    factor = lax.rsqrt(jnp.mean(wide * wide, axis=-1, keepdims=True) + norm_eps)
    return wide * factor * gain


def halves(g):
    hi = g.astype(bf16)
    mid = (g - hi.astype(f32)).astype(bf16)
    return jnp.concatenate([hi, mid], axis=0)


def each_prompt(rows, prompts):
    row_prompt = lax.broadcasted_iota(jnp.int32, (rows.shape[0], 1), 0) % prompts
    zero = jnp.zeros_like(rows)
    return jnp.concatenate([jnp.where(row_prompt == p, rows, zero) for p in range(prompts)], axis=1)


def by_prompt(table, row_prompt, prompts):
    picked = table[0:1]
    for p in range(1, prompts):
        picked = jnp.where(row_prompt == p, table[p : p + 1], picked)
    return picked


def main_kernel(
    own_pos, prompts, heads, kv, dec_own,
    x_hbm, dec_ref, wq_hbm, wk_hbm, wv_hbm, wd_hbm, bias_ref, gain_ref, head_gain_ref, mk_ref, mq_ref, ps_ref, ds_hbm,
    nrm_hbm, ndec_hbm, po_ref, cols_ref, vrow_ref,
    xb, nb, nd, wq, wk, wv, wd, qs, ks, vs, gs, sq, ek, es, oi, tots, later, st, loc, rx, inc, sin, tb, rxt, ttr,
    sbuf, qet, attb, dl,
    x_sem, w_sem, n_send, n_recv, nd_send, nd_recv, p1_send, p1_recv, t_send, t_recv, p2_send, p2_recv,
    s_sem, out_local, out_send, out_recv, d_local, d_send, d_recv,
):
    me = lax.axis_index("tp")
    other = 1 - me
    here = lax.axis_index("kv")
    own = own_pos * prompts
    rows_all = 2 * own
    chunk = min(256, own)
    count = own // chunk
    n = STEP * prompts
    half = n // 2
    blocks = rows_all // n
    group = 2 if heads % 2 == 0 else 1
    groups = heads // group
    gk, gv = group * DK, group * DV
    qk, vw = heads * DK, heads * DV
    part = DK // kv
    seqs = 2 * dec_own
    pos = chunk // prompts

    def x_copy(j):
        at = pl.ds(j * pos, pos)
        return pltpu.make_async_copy(x_hbm.at[at], xb.at[at], x_sem.at[j])

    for j in range(count):
        x_copy(j).start()
    loads = []
    for i in range(groups):
        kc, vc = pl.ds(i * gk, gk), pl.ds(i * gv, gv)
        for s, (src, dst, cols) in enumerate(((wk_hbm, wk, kc), (wd_hbm, wd, kc), (wv_hbm, wv, vc))):
            loads.append(pltpu.make_async_copy(src.at[:, cols], dst.at[:, cols], w_sem.at[3 * i + s]))
    loads.append(pltpu.make_async_copy(wq_hbm, wq, w_sem.at[3 * groups]))
    for load in loads:
        load.start()

    barrier = pltpu.get_barrier_semaphore()
    pl.semaphore_signal(barrier, inc=1, device_id={"tp": other}, device_id_type=MESH)
    for d in range(1, kv):
        pl.semaphore_signal(barrier, inc=1, device_id={"kv": lax.rem(here + d, kv)}, device_id_type=MESH)
    pl.semaphore_wait(barrier, kv)

    def state_copy(h):
        return pltpu.make_async_copy(ds_hbm.at[:, h], sbuf.at[h % 2], s_sem.at[h])

    def piece_copy(j, side):
        rows = pl.ds(pl.multiple_of(side * own + j * chunk, chunk), chunk)
        return pltpu.make_async_remote_copy(
            src_ref=nb.at[rows], dst_ref=nb.at[rows], send_sem=n_send.at[j], recv_sem=n_recv.at[j],
            device_id={"tp": other}, device_id_type=MESH,
        )

    mine = pl.ds(pl.multiple_of(me * PAD, PAD), PAD)
    theirs = pl.ds(pl.multiple_of(other * PAD, PAD), PAD)
    dec_rows = normed(dec_ref[...], gain_ref[...])
    nd[mine, :] = jnp.concatenate([dec_rows, jnp.zeros((PAD - dec_own, dec_rows.shape[1]), f32)], axis=0).astype(bf16)
    dec_copy = pltpu.make_async_remote_copy(
        src_ref=nd.at[mine], dst_ref=nd.at[mine], send_sem=nd_send, recv_sem=nd_recv,
        device_id={"tp": other}, device_id_type=MESH,
    )
    small = min(32, pos)
    for j in range(count):
        x_copy(j).wait()

        @pl.loop(0, pos // small)
        def _(s):
            at = pl.multiple_of(j * pos + s * small, small)
            rows = xb[pl.ds(at, small)].reshape(small * prompts, xb.shape[2])
            to = pl.ds(pl.multiple_of(me * own + at * prompts, small * prompts), small * prompts)
            nb[to, :] = normed(rows, gain_ref[...]).astype(bf16)

        if j == 0:
            dec_copy.start()
        else:
            piece_copy(j - 1, me).start()
    piece_copy(count - 1, me).start()

    def decay_of(product, i):
        at = pl.ds(pl.multiple_of(me * qk + i * gk, gk), product.shape[1])
        t = product + bias_ref[:, at]
        return (jnp.minimum(t, 0.0) - jnp.log1p(jnp.exp(-jnp.abs(t)))) * (1.0 / decay_tau)

    def project(at, i):
        rows = pl.ds(pl.multiple_of(at, chunk), chunk)
        kc, vc = slice(i * gk, (i + 1) * gk), slice(i * gv, (i + 1) * gv)
        block = nb[rows, :]
        ks[rows, kc] = dot(block, wk[:, kc]).astype(bf16)
        vs[rows, vc] = dot(block, wv[:, vc]).astype(bf16)
        gs[rows, kc] = decay_of(dot(block, wd[:, kc]), i)

    row_prompt = lax.broadcasted_iota(jnp.int32, (n, 1), 0) % prompts

    def keys_of(i):
        kc = slice(i * gk, (i + 1) * gk)
        later[:, kc] = jnp.zeros((8, gk), f32)

        @pl.loop(0, blocks)
        def _(back):
            at = blocks - 1 - back
            rows = pl.ds(pl.multiple_of(at * n, n), n)
            sums = dot(mk_ref[...], halves(gs[rows, kc]))
            end = ks[rows, kc].astype(f32) * jnp.exp(sums[:n])
            ek[rows, kc] = end.astype(bf16)
            after = later[:, kc]
            es[rows, :] = (end * by_prompt(jnp.exp(after), row_prompt, prompts)).astype(bf16)
            total = sums[n : n + 8]
            tots[at, :, kc] = total
            later[:, kc] = after + total

        span = min(512, rows_all)
        for hh in range(group):
            h = i * group + hh
            hk, hv = slice(hh * DK, (hh + 1) * DK), slice(h * DV, (h + 1) * DV)
            st[h] = jnp.zeros(st.shape[1:], f32)

            @pl.loop(0, rows_all // span)
            def _(c):
                rows = pl.ds(pl.multiple_of(c * span, span), span)
                st[h] = st[h] + dot_tn(each_prompt(es[rows, hk], prompts), vs[rows, hv])

            for p in range(prompts):
                loc[h * prompts + p] = st[h, p * DK : (p + 1) * DK, :].astype(bf16)
                tb[i, hh * prompts + p : hh * prompts + p + 1, :] = later[p : p + 1, h * DK : (h + 1) * DK]
            for d in range(1, kv):
                local_copy(d, h).start()
        for d in range(1, kv):
            total_copy(d, i).start()

    def local_copy(d, h):
        to = lax.rem(here + d, kv)
        hp = pl.ds(h * prompts, prompts)
        return pltpu.make_async_remote_copy(
            src_ref=loc.at[hp, pl.ds(pl.multiple_of(to * part, part), part)], dst_ref=rx.at[d, hp],
            send_sem=p1_send.at[d, h], recv_sem=p1_recv.at[d, h], device_id={"kv": to}, device_id_type=MESH,
        )

    def total_copy(d, i):
        return pltpu.make_async_remote_copy(
            src_ref=tb.at[i], dst_ref=rxt.at[d, i], send_sem=t_send.at[d, i], recv_sem=t_recv.at[d, i],
            device_id={"kv": lax.rem(here + d, kv)}, device_id_type=MESH,
        )

    def incoming_copy(d, i):
        to = lax.rem(here + d, kv)
        hp = pl.ds(i * group * prompts, group * prompts)
        return pltpu.make_async_remote_copy(
            src_ref=inc.at[to, hp], dst_ref=sin.at[hp, pl.ds(pl.multiple_of(here * part, part), part)],
            send_sem=p2_send.at[d, i], recv_sem=p2_recv.at[d, i], device_id={"kv": to}, device_id_type=MESH,
        )

    my_part = pl.ds(pl.multiple_of(here * part, part), part)

    def pass_on(i):
        for d in range(1, kv):
            total_copy(d, i).wait_recv()
            for hh in range(group):
                local_copy(d, i * group + hh).wait_recv()
        rxt[0, i] = tb[i]
        for hh in range(group):
            for p in range(prompts):
                hp = (i * group + hh) * prompts + p
                rx[0, hp] = loc[hp, my_part, :]
        for c in range(kv):
            d = lax.rem(here - c + kv, kv)
            ttr[c] = jnp.transpose(jnp.exp(rxt[d, i]))
        for hh in range(group):
            h = i * group + hh
            for p in range(prompts):
                hp = h * prompts + p
                running = ps_ref[p, h]
                for c in range(kv):
                    d = lax.rem(here - c + kv, kv)
                    inc[c, hp] = running.astype(bf16)
                    at = hh * prompts + p
                    running = running * ttr[c, my_part, at : at + 1] + rx[d, hp].astype(f32)
                po_ref[p, h] = running
        for d in range(1, kv):
            incoming_copy(d, i).start()
        for hh in range(group):
            for p in range(prompts):
                hp = (i * group + hh) * prompts + p
                sin[hp, my_part, :] = inc[here, hp]

    for i in range(groups):
        for s in range(3):
            loads[3 * i + s].wait()
        if i == 0:
            @pl.loop(0, count)
            def _(j):
                project(me * own + j * chunk, 0)

            @pl.loop(0, count)
            def _(j):
                piece_copy(j, other).wait_recv()
                project(other * own + j * chunk, 0)

            for h in range(min(2, heads)):
                state_copy(h).start()
        else:
            @pl.loop(0, 2 * count)
            def _(j):
                project(j * chunk, i)
        keys_of(i)

    loads[3 * groups].wait()

    @pl.loop(0, 2 * count)
    def _(j):
        rows = pl.ds(pl.multiple_of(j * chunk, chunk), chunk)
        qs[rows, :] = (dot(nb[rows, :], wq[...]) * DK ** (-0.5)).astype(bf16)

    for j in range(count):
        piece_copy(j, me).wait_send()
    dec_copy.wait()

    r_at = lax.broadcasted_iota(jnp.int32, (n, n), 0)
    c_at = lax.broadcasted_iota(jnp.int32, (n, n), 1)

    def inside(block):
        rows = pl.ds(pl.multiple_of(block * n, n), n)
        keep = (c_at <= r_at) & (r_at % prompts == c_at % prompts)
        for i in range(groups):
            kc = slice(i * gk, (i + 1) * gk)
            sums = dot(mq_ref[...], halves(gs[rows, kc]))
            b, d0, d1 = sums[:n], sums[n : n + half], sums[n + half :]
            q = qs[rows, kc].astype(f32)
            k = ks[rows, kc].astype(f32)
            sq[rows, kc] = (q * jnp.exp(b)).astype(bf16)
            near_q0 = (q[:half] * jnp.exp(d0)).astype(bf16)
            near_k0 = (k[:half] * jnp.exp(-d0)).astype(bf16)
            near_q1 = (q[half:] * jnp.exp(d1[half:])).astype(bf16)
            near_k1 = (k * jnp.exp(-d1)).astype(bf16)
            for hh in range(group):
                hk = slice(hh * DK, (hh + 1) * DK)
                hv = slice((i * group + hh) * DV, (i * group + hh + 1) * DV)
                v = vs[rows, hv]
                w0 = jnp.where(keep[:half, :half], dot_nt(near_q0[:, hk], near_k0[:, hk]), 0.0).astype(bf16)
                w1 = jnp.where(keep[half:], dot_nt(near_q1[:, hk], near_k1[:, hk]), 0.0).astype(bf16)
                oi[rows, hv] = jnp.concatenate([dot(w0, v[:half]), dot(w1, v)], axis=0).astype(bf16)

    pass_on(0)

    @pl.loop(0, blocks // 2)
    def _(block):
        inside(block)

    for i in range(1, groups):
        pass_on(i)

    @pl.loop(blocks // 2, blocks)
    def _(block):
        inside(block)

    def head_norm(block, h):
        factor = lax.rsqrt(jnp.mean(block * block, axis=-1, keepdims=True) + norm_eps)
        at = pl.ds(pl.multiple_of(me * vw + h * DV, DV), DV)
        return (block * factor * head_gain_ref[:, at]).astype(bf16)

    new = nd[...]
    q_d = (dot(new, wq[...]) * DK ** (-0.5)).astype(bf16).astype(f32)
    k_d = dot(new, wk[...]).astype(bf16).astype(f32)
    e_d = jnp.exp(decay_of(dot(new, wd[...]), 0))
    vrow_ref[...] = dot(new, wv[...]).astype(bf16).astype(f32)
    for h in range(heads):
        at = slice(h * DK, (h + 1) * DK)
        qet[h] = jnp.transpose(q_d[:, at] * e_d[:, at])
        cols_ref[0, h] = jnp.transpose(e_d[:, at])
        cols_ref[1, h] = jnp.transpose(k_d[:, at])
    attb[...] = jnp.zeros_like(attb)
    for h in range(heads):
        state_copy(h).wait()
        for s in range(seqs):
            row = (s // dec_own) * PAD + s % dec_own
            attb[row : row + 1, h * DV : (h + 1) * DV] = jnp.sum(
                sbuf[h % 2, s] * qet[h, :, row : row + 1], axis=0, keepdims=True
            )
        if h + 2 < heads:
            state_copy(h + 2).start()
    for h in range(heads):
        at, hv = slice(h * DK, (h + 1) * DK), slice(h * DV, (h + 1) * DV)
        score = jnp.sum(q_d[:, at] * k_d[:, at], axis=-1, keepdims=True)
        dl[:, hv] = head_norm(attb[:, hv] + score * vrow_ref[:, hv], h)
    my_cols = pl.ds(pl.multiple_of(me * vw, vw), vw)
    dec_keep = pltpu.make_async_copy(dl.at[mine], ndec_hbm.at[:, my_cols], d_local)
    dec_keep.start()
    dec_give = pltpu.make_async_remote_copy(
        src_ref=dl.at[theirs], dst_ref=ndec_hbm.at[:, my_cols], send_sem=d_send, recv_sem=d_recv,
        device_id={"tp": other}, device_id_type=MESH,
    )
    dec_give.start()

    def out_refs(side, j, i):
        rows = pl.ds(pl.multiple_of(side * own + j * n, n), n)
        cols = pl.ds(pl.multiple_of(me * vw + i * gv, gv), gv)
        return oi.at[rows, pl.ds(i * gv, gv)], nrm_hbm.at[pl.ds(pl.multiple_of(j * n, n), n), cols]

    def keep_copy(j, i):
        src, dst = out_refs(me, j, i)
        return pltpu.make_async_copy(src, dst, out_local.at[i, j])

    def give_copy(j, i):
        src, dst = out_refs(other, j, i)
        return pltpu.make_async_remote_copy(
            src_ref=src, dst_ref=dst, send_sem=out_send.at[i, j], recv_sem=out_recv.at[i, j],
            device_id={"tp": other}, device_id_type=MESH,
        )

    for i in range(groups):
        for d in range(1, kv):
            incoming_copy(d, i).wait_recv()
        for hh in range(group):
            h = i * group + hh
            for p in range(prompts):
                st[h, p * DK : (p + 1) * DK, :] = sin[h * prompts + p].astype(f32)

        @pl.loop(0, blocks)
        def _(block):
            rows = pl.ds(pl.multiple_of(block * n, n), n)
            for hh in range(group):
                h = i * group + hh
                hk, hv = slice(h * DK, (h + 1) * DK), slice(h * DV, (h + 1) * DV)
                state = st[h]
                from_state = dot(each_prompt(sq[rows, hk], prompts), state.astype(bf16))
                oi[rows, hv] = head_norm(oi[rows, hv].astype(f32) + from_state, h)
                added = dot_tn(each_prompt(ek[rows, hk], prompts), vs[rows, hv])
                decay = jnp.transpose(jnp.exp(tots[block, :, hk]))
                for p in range(prompts):
                    at = slice(p * DK, (p + 1) * DK)
                    st[h, at, :] = state[at] * decay[:, p : p + 1] + added[at]
            side = block // (blocks // 2)
            j = block - side * (blocks // 2)

            @pl.when(side == me)
            def _():
                keep_copy(j, i).start()

            @pl.when(side != me)
            def _():
                give_copy(j, i).start()

    for d in range(1, kv):
        for h in range(heads):
            local_copy(d, h).wait_send()
        for i in range(groups):
            total_copy(d, i).wait_send()
            incoming_copy(d, i).wait_send()
    dec_keep.wait()
    dec_give.wait()
    for i in range(groups):
        @pl.loop(0, blocks // 2)
        def _(j):
            keep_copy(j, i).wait()
            give_copy(j, i).wait_send()
            give_copy(j, i).wait_recv()


def last_kernel(
    own_pos, prompts, heads, dec_own,
    nrm_hbm, ndec_ref, w_hbm, ds_hbm, cols_ref, vrow_ref, ps_ref,
    y_hbm, yd_ref, po_ref, do_hbm,
    nrm, w, yb, sb,
    n_sem, w_sem, s_sem, y_sem, o_sem,
):
    own = own_pos * prompts
    chunk = min(256, own)
    count = own // chunk
    pos = chunk // prompts
    width = w.shape[1]
    tile = width // heads
    seqs = 2 * dec_own

    def n_copy(j):
        at = pl.ds(j * chunk, chunk)
        return pltpu.make_async_copy(nrm_hbm.at[at], nrm.at[at], n_sem.at[j])

    def w_copy(t):
        at = pl.ds(t * tile, tile)
        return pltpu.make_async_copy(w_hbm.at[:, at], w.at[:, at], w_sem.at[t])

    def s_copy(h):
        return pltpu.make_async_copy(ds_hbm.at[:, h], sb.at[h], s_sem.at[h])

    def o_copy(h):
        return pltpu.make_async_copy(sb.at[h], do_hbm.at[:, h], o_sem.at[h])

    def y_copy(t):
        at = pl.ds(t * tile, tile)
        return pltpu.make_async_copy(yb.at[:, :, at], y_hbm.at[:, :, at], y_sem.at[t])

    n_copy(0).start()
    w_copy(0).start()
    for j in range(1, count):
        n_copy(j).start()
    s_copy(0).start()
    for t in range(1, heads):
        w_copy(t).start()
        s_copy(t).start()
    po_ref[...] = ps_ref[...]
    for t in range(heads):
        at = slice(t * tile, (t + 1) * tile)
        w_copy(t).wait()
        s_copy(t).wait()
        each = -(-seqs // count)
        for j in range(count):
            if t == 0:
                n_copy(j).wait()
            block = dot(nrm[j * chunk : (j + 1) * chunk, :], w[:, at]).astype(bf16)
            yb[j * pos : (j + 1) * pos, :, at] = block.reshape(pos, prompts, tile)
            for s in range(j * each, min(seqs, (j + 1) * each)):
                row = (s // dec_own) * PAD + s % dec_own
                v = vrow_ref[row : row + 1, t * DV : (t + 1) * DV]
                sb[t, s] = sb[t, s] * cols_ref[0, t, :, row : row + 1] + cols_ref[1, t, :, row : row + 1] * v
        yd_ref[:, at] = dot(ndec_ref[...], w[:, at])[:dec_own].astype(bf16)
        y_copy(t).start()
        o_copy(t).start()
    for t in range(heads):
        y_copy(t).wait()
        o_copy(t).wait()


ANY = pl.BlockSpec(memory_space=pl.ANY)
VMEM = pl.BlockSpec(memory_space=pltpu.VMEM)
LIMIT = 62 * 1024 * 1024


def on_device(
    pieces, new_tokens, w_query, w_key, w_value, w_decay, decay_bias, norm_gain, head_gain, w_out, prompt_state, decode_state,
):
    kv = lax.axis_size("kv")
    qk = w_query.shape[1]
    heads = qk // DK
    vw = heads * DV
    own_pos, prompts, width = pieces.shape
    own = own_pos * prompts
    chunk = min(256, own)
    count = own // chunk
    rows = 2 * own
    blocks = rows // (STEP * prompts)
    dec_own = new_tokens.shape[0]
    seqs = 2 * dec_own
    part = DK // kv
    group = 2 if heads % 2 == 0 else 1
    groups = heads // group
    hp = heads * prompts
    mk, mq = (jnp.asarray(m, bf16) for m in sum_matrices(prompts))
    dma = pltpu.SemaphoreType.DMA
    nrm, ndec, prompt_out, cols, v_rows = pl.pallas_call(
        functools.partial(main_kernel, own_pos, prompts, heads, kv, dec_own),
        name="layer",
        out_shape=(
            jax.ShapeDtypeStruct((own, 2 * vw), bf16),
            jax.ShapeDtypeStruct((PAD, 2 * vw), bf16),
            jax.ShapeDtypeStruct(prompt_state.shape, f32),
            jax.ShapeDtypeStruct((2, heads, DK, 2 * PAD), f32),
            jax.ShapeDtypeStruct((2 * PAD, vw), f32),
        ),
        in_specs=[ANY, VMEM, ANY, ANY, ANY, ANY, VMEM, VMEM, VMEM, VMEM, VMEM, VMEM, ANY],
        out_specs=(ANY, ANY, VMEM, VMEM, VMEM),
        scratch_shapes=[
            pltpu.VMEM(pieces.shape, bf16),
            pltpu.VMEM((rows, width), bf16),
            pltpu.VMEM((2 * PAD, width), bf16),
            pltpu.VMEM((width, qk), bf16),
            pltpu.VMEM((width, qk), bf16),
            pltpu.VMEM((width, vw), bf16),
            pltpu.VMEM((width, qk), bf16),
            pltpu.VMEM((rows, qk), bf16),
            pltpu.VMEM((rows, qk), bf16),
            pltpu.VMEM((rows, vw), bf16),
            pltpu.VMEM((rows, qk), f32),
            pltpu.VMEM((rows, qk), bf16),
            pltpu.VMEM((rows, qk), bf16),
            pltpu.VMEM((rows, group * DK), bf16),
            pltpu.VMEM((rows, vw), bf16),
            pltpu.VMEM((blocks, 8, qk), f32),
            pltpu.VMEM((8, qk), f32),
            pltpu.VMEM((heads, prompts * DK, DV), f32),
            pltpu.VMEM((hp, DK, DV), bf16),
            pltpu.VMEM((kv, hp, part, DV), bf16),
            pltpu.VMEM((kv, hp, part, DV), bf16),
            pltpu.VMEM((hp, DK, DV), bf16),
            pltpu.VMEM((groups, 8, DK), f32),
            pltpu.VMEM((kv, groups, 8, DK), f32),
            pltpu.VMEM((kv, DK, 8), f32),
            pltpu.VMEM((2, seqs, DK, DV), f32),
            pltpu.VMEM((heads, DK, 2 * PAD), f32),
            pltpu.VMEM((2 * PAD, vw), f32),
            pltpu.VMEM((2 * PAD, vw), bf16),
            dma((count,)),
            dma((3 * groups + 1,)),
            dma((count,)),
            dma((count,)),
            dma,
            dma,
            dma((kv, heads)),
            dma((kv, heads)),
            dma((kv, groups)),
            dma((kv, groups)),
            dma((kv, groups)),
            dma((kv, groups)),
            dma((heads,)),
            dma((groups, blocks // 2)),
            dma((groups, blocks // 2)),
            dma((groups, blocks // 2)),
            dma,
            dma,
            dma,
        ],
        compiler_params=pltpu.CompilerParams(collective_id=0, has_side_effects=True, vmem_limit_bytes=LIMIT),
    )(
        pieces, new_tokens, w_query, w_key, w_value, w_decay, decay_bias[None], norm_gain[None], head_gain[None],
        mk, mq, prompt_state, decode_state,
    )
    return pl.pallas_call(
        functools.partial(last_kernel, own_pos, prompts, heads, dec_own),
        name="last",
        out_shape=(
            jax.ShapeDtypeStruct(pieces.shape, bf16),
            jax.ShapeDtypeStruct(new_tokens.shape, bf16),
            jax.ShapeDtypeStruct(prompt_state.shape, f32),
            jax.ShapeDtypeStruct(decode_state.shape, f32),
        ),
        in_specs=[ANY, VMEM, ANY, ANY, VMEM, VMEM, VMEM],
        out_specs=(ANY, VMEM, VMEM, ANY),
        scratch_shapes=[
            pltpu.VMEM((own, 2 * vw), bf16),
            pltpu.VMEM(w_out.shape, bf16),
            pltpu.VMEM(pieces.shape, bf16),
            pltpu.VMEM((heads, seqs, DK, DV), f32),
            dma((count,)),
            dma((heads,)),
            dma((heads,)),
            dma((heads,)),
            dma((heads,)),
        ],
        compiler_params=pltpu.CompilerParams(vmem_limit_bytes=LIMIT),
    )(nrm, ndec, w_out, decode_state, cols, v_rows, prompt_out)


def solution(mesh):
    return jax.shard_map(
        on_device,
        mesh=mesh,
        in_specs=(
            P(("kv", "tp"), "dp", None),
            P(("dp", "kv", "tp"), None),
            P(None, "tp"),
            P(None, "tp"),
            P(None, "tp"),
            P(None, "tp"),
            P(),
            P(),
            P(),
            P(),
            P("dp", "tp", "kv", None),
            P(("dp", "kv"), "tp", None, None),
        ),
        out_specs=(
            P(("kv", "tp"), "dp", None),
            P(("dp", "kv", "tp"), None),
            P("dp", "tp", "kv", None),
            P(("dp", "kv"), "tp", None, None),
        ),
        check_vma=False,
    )
```

```python
import functools

import jax
import jax.numpy as jnp
import numpy as np
from jax import lax
from jax.experimental import pallas as pl
from jax.experimental.pallas import tpu as pltpu
from jax.sharding import PartitionSpec as P

DK = 128
DV = 256
STEP = 64
PART = 16

norm_eps = 0.1
decay_tau = 16.0
f32, bf16 = jnp.float32, jnp.bfloat16
MESH = pl.DeviceIdType.MESH
PAD = 16


def dot(a, b):
    return jnp.dot(a, b, preferred_element_type=f32)


def dot_nt(a, b):
    return lax.dot_general(a, b, (((1,), (1,)), ((), ())), preferred_element_type=f32)


def dot_tn(a, b):
    return lax.dot_general(a, b, (((0,), (0,)), ((), ())), preferred_element_type=f32)


def sum_matrices(prompts):
    n = STEP * prompts
    r, c = np.arange(n)[:, None], np.arange(n)[None]
    same = (r % prompts) == (c % prompts)

    def from_anchor(edge):
        return (same & (c >= edge) & (c <= r)) * 1.0 - (same & (c < edge) & (c > r)) * 1.0

    b = (same & (c <= r)) * 1.0
    rest = (same & (c > r)) * 1.0
    whole = ((np.arange(16)[:, None] == (c % prompts))) * 1.0
    d0 = from_anchor(PART * prompts)[: n // 2]
    d1 = from_anchor(3 * PART * prompts)
    for_keys = np.concatenate([rest, whole], axis=0)
    near = np.concatenate([b, d0, d1], axis=0)
    return np.concatenate([for_keys] * 2, axis=1), np.concatenate([near] * 2, axis=1)


def normed(rows, gain):
    wide = rows.astype(f32)
    factor = lax.rsqrt(jnp.mean(wide * wide, axis=-1, keepdims=True) + norm_eps)
    return wide * factor * gain


def halves(g):
    hi = g.astype(bf16)
    mid = (g - hi.astype(f32)).astype(bf16)
    return jnp.concatenate([hi, mid], axis=0)


def each_prompt(rows, prompts):
    row_prompt = lax.broadcasted_iota(jnp.int32, (rows.shape[0], 1), 0) % prompts
    zero = jnp.zeros_like(rows)
    return jnp.concatenate([jnp.where(row_prompt == p, rows, zero) for p in range(prompts)], axis=1)


def turned(rows, prompts):
    columns = jnp.transpose(rows)
    column_prompt = lax.broadcasted_iota(jnp.int32, (1, columns.shape[1]), 1) % prompts
    zero = jnp.zeros_like(columns)
    return jnp.concatenate([jnp.where(column_prompt == p, columns, zero) for p in range(prompts)], axis=0)


def by_prompt(table, row_prompt, prompts):
    picked = table[0:1]
    for p in range(1, prompts):
        picked = jnp.where(row_prompt == p, table[p : p + 1], picked)
    return picked


def main_kernel(
    own_pos, prompts, heads, kv, dec_own,
    x_hbm, dec_ref, wq_hbm, wk_hbm, wv_hbm, wd_hbm, bias_ref, gain_ref, head_gain_ref, mk_ref, mq_ref, ps_ref, ds_hbm,
    nrm_hbm, ndec_hbm, po_ref, cols_ref, vrow_ref,
    xb, nb, nd, wq, wk, wv, wd, qs, ks, vs, gs, sq, ek, es, oi, tots, later, st, loc, rx, inc, sin, tb, rxt, ttr,
    sbuf, qet, attb, dl,
    x_sem, w_sem, n_send, n_recv, nd_send, nd_recv, p1_send, p1_recv, t_send, t_recv, p2_send, p2_recv,
    s_sem, out_local, out_send, out_recv, d_local, d_send, d_recv,
):
    me = lax.axis_index("tp")
    other = 1 - me
    here = lax.axis_index("kv")
    own = own_pos * prompts
    rows_all = 2 * own
    chunk = min(256, own)
    count = own // chunk
    n = STEP * prompts
    half = n // 2
    blocks = rows_all // n
    group = 2 if heads % 2 == 0 else 1
    groups = heads // group
    gk, gv = group * DK, group * DV
    qk, vw = heads * DK, heads * DV
    part = DK // kv
    seqs = 2 * dec_own
    pos = chunk // prompts

    def x_copy(j):
        at = pl.ds(j * pos, pos)
        return pltpu.make_async_copy(x_hbm.at[at], xb.at[at], x_sem.at[j])

    for j in range(count):
        x_copy(j).start()
    loads = []
    for i in range(groups):
        kc, vc = pl.ds(i * gk, gk), pl.ds(i * gv, gv)
        for s, (src, dst, cols) in enumerate(((wk_hbm, wk, kc), (wd_hbm, wd, kc), (wv_hbm, wv, vc))):
            loads.append(pltpu.make_async_copy(src.at[:, cols], dst.at[:, cols], w_sem.at[3 * i + s]))
    loads.append(pltpu.make_async_copy(wq_hbm, wq, w_sem.at[3 * groups]))
    for load in loads:
        load.start()

    barrier = pltpu.get_barrier_semaphore()
    pl.semaphore_signal(barrier, inc=1, device_id={"tp": other}, device_id_type=MESH)
    for d in range(1, kv):
        pl.semaphore_signal(barrier, inc=1, device_id={"kv": lax.rem(here + d, kv)}, device_id_type=MESH)
    pl.semaphore_wait(barrier, kv)

    def state_copy(h):
        return pltpu.make_async_copy(ds_hbm.at[:, h], sbuf.at[h % 2], s_sem.at[h])

    def piece_copy(j, side):
        rows = pl.ds(pl.multiple_of(side * own + j * chunk, chunk), chunk)
        return pltpu.make_async_remote_copy(
            src_ref=nb.at[rows], dst_ref=nb.at[rows], send_sem=n_send.at[j], recv_sem=n_recv.at[j],
            device_id={"tp": other}, device_id_type=MESH,
        )

    mine = pl.ds(pl.multiple_of(me * PAD, PAD), PAD)
    theirs = pl.ds(pl.multiple_of(other * PAD, PAD), PAD)
    dec_rows = normed(dec_ref[...], gain_ref[...])
    nd[mine, :] = jnp.concatenate([dec_rows, jnp.zeros((PAD - dec_own, dec_rows.shape[1]), f32)], axis=0).astype(bf16)
    dec_copy = pltpu.make_async_remote_copy(
        src_ref=nd.at[mine], dst_ref=nd.at[mine], send_sem=nd_send, recv_sem=nd_recv,
        device_id={"tp": other}, device_id_type=MESH,
    )
    small = min(32, pos)
    for j in range(count):
        x_copy(j).wait()

        @pl.loop(0, pos // small)
        def _(s):
            at = pl.multiple_of(j * pos + s * small, small)
            to = pl.ds(pl.multiple_of(me * own + at * prompts, small * prompts), small * prompts)
            nb[to, :] = xb[pl.ds(at, small)].reshape(small * prompts, xb.shape[2])
            nb[to, :] = normed(nb[to, :], gain_ref[...]).astype(bf16)

        if j == 0:
            dec_copy.start()
        else:
            piece_copy(j - 1, me).start()
    piece_copy(count - 1, me).start()

    def decay_of(product, i):
        at = pl.ds(pl.multiple_of(me * qk + i * gk, gk), product.shape[1])
        t = product + bias_ref[:, at]
        return (jnp.minimum(t, 0.0) - jnp.log1p(jnp.exp(-jnp.abs(t)))) * (1.0 / decay_tau)

    wide = min(512, own)

    def project(at, i):
        rows = pl.ds(pl.multiple_of(at, wide), wide)
        kc, vc = slice(i * gk, (i + 1) * gk), slice(i * gv, (i + 1) * gv)
        block = nb[rows, :]
        ks[rows, kc] = dot(block, wk[:, kc]).astype(bf16)
        vs[rows, vc] = dot(block, wv[:, vc]).astype(bf16)
        gs[rows, kc] = decay_of(dot(block, wd[:, kc]), i)

    row_prompt = lax.broadcasted_iota(jnp.int32, (n, 1), 0) % prompts

    def keys_of(i):
        kc = slice(i * gk, (i + 1) * gk)
        later[:, kc] = jnp.zeros((8, gk), f32)

        batch = 4 if blocks % 4 == 0 else 1

        @pl.loop(0, blocks // batch)
        def _(back):
            after = later[:, kc]
            for u in range(batch):
                at = blocks - 1 - back * batch - u
                rows = pl.ds(pl.multiple_of(at * n, n), n)
                sums = dot(mk_ref[...], halves(gs[rows, kc]))
                end = ks[rows, kc].astype(f32) * jnp.exp(sums[:n])
                ek[rows, kc] = end.astype(bf16)
                es[rows, :] = (end * by_prompt(jnp.exp(after), row_prompt, prompts)).astype(bf16)
                total = sums[n : n + 8]
                tots[at, :, kc] = total
                after = after + total
            later[:, kc] = after

        span = min(512, rows_all)
        for hh in range(group):
            st[i * group + hh] = jnp.zeros(st.shape[1:], f32)

        @pl.loop(0, rows_all // span)
        def _(c):
            rows = pl.ds(pl.multiple_of(c * span, span), span)
            for hh in range(group):
                h = i * group + hh
                st[h] = st[h] + dot(turned(es[rows, hh * DK : (hh + 1) * DK], prompts), vs[rows, h * DV : (h + 1) * DV])

        for hh in range(group):
            h = i * group + hh
            for p in range(prompts):
                loc[h * prompts + p] = st[h, p * DK : (p + 1) * DK, :].astype(bf16)
                tb[i, hh * prompts + p : hh * prompts + p + 1, :] = later[p : p + 1, h * DK : (h + 1) * DK]
            for d in range(1, kv):
                local_copy(d, h).start()
        for d in range(1, kv):
            total_copy(d, i).start()

    def local_copy(d, h):
        to = lax.rem(here + d, kv)
        hp = pl.ds(h * prompts, prompts)
        return pltpu.make_async_remote_copy(
            src_ref=loc.at[hp, pl.ds(pl.multiple_of(to * part, part), part)], dst_ref=rx.at[d, hp],
            send_sem=p1_send.at[d, h], recv_sem=p1_recv.at[d, h], device_id={"kv": to}, device_id_type=MESH,
        )

    def total_copy(d, i):
        return pltpu.make_async_remote_copy(
            src_ref=tb.at[i], dst_ref=rxt.at[d, i], send_sem=t_send.at[d, i], recv_sem=t_recv.at[d, i],
            device_id={"kv": lax.rem(here + d, kv)}, device_id_type=MESH,
        )

    def incoming_copy(d, i):
        to = lax.rem(here + d, kv)
        hp = pl.ds(i * group * prompts, group * prompts)
        return pltpu.make_async_remote_copy(
            src_ref=inc.at[to, hp], dst_ref=sin.at[hp, pl.ds(pl.multiple_of(here * part, part), part)],
            send_sem=p2_send.at[d, i], recv_sem=p2_recv.at[d, i], device_id={"kv": to}, device_id_type=MESH,
        )

    my_part = pl.ds(pl.multiple_of(here * part, part), part)

    def pass_on(i):
        for d in range(1, kv):
            total_copy(d, i).wait_recv()
            for hh in range(group):
                local_copy(d, i * group + hh).wait_recv()
        rxt[0, i] = tb[i]
        for hh in range(group):
            for p in range(prompts):
                hp = (i * group + hh) * prompts + p
                rx[0, hp] = loc[hp, my_part, :]
        for c in range(kv):
            d = lax.rem(here - c + kv, kv)
            ttr[c] = jnp.transpose(jnp.exp(rxt[d, i]))
        for hh in range(group):
            h = i * group + hh
            for p in range(prompts):
                hp = h * prompts + p
                running = ps_ref[p, h]
                for c in range(kv):
                    d = lax.rem(here - c + kv, kv)
                    inc[c, hp] = running.astype(bf16)
                    at = hh * prompts + p
                    running = running * ttr[c, my_part, at : at + 1] + rx[d, hp].astype(f32)
                po_ref[p, h] = running
        for d in range(1, kv):
            incoming_copy(d, i).start()
        for hh in range(group):
            for p in range(prompts):
                hp = (i * group + hh) * prompts + p
                sin[hp, my_part, :] = inc[here, hp]

    for i in range(groups):
        for s in range(3):
            loads[3 * i + s].wait()
        if i == 0:
            @pl.loop(0, own // wide)
            def _(j):
                project(me * own + j * wide, 0)

            @pl.loop(0, own // wide)
            def _(j):
                for c in range(wide // chunk):
                    piece_copy(j * (wide // chunk) + c, other).wait_recv()
                project(other * own + j * wide, 0)

            for h in range(min(2, heads)):
                state_copy(h).start()
        else:
            @pl.loop(0, rows_all // wide)
            def _(j):
                @pl.when(j == rows_all // wide - 1)
                def _():
                    pass_on(i - 1)

                project(j * wide, i)
        keys_of(i)

    loads[3 * groups].wait()

    @pl.loop(0, rows_all // wide)
    def _(j):
        rows = pl.ds(pl.multiple_of(j * wide, wide), wide)
        qs[rows, :] = (dot(nb[rows, :], wq[...]) * DK ** (-0.5)).astype(bf16)

    for j in range(count):
        piece_copy(j, me).wait_send()
    dec_copy.wait()

    r_at = lax.broadcasted_iota(jnp.int32, (n, n), 0)
    c_at = lax.broadcasted_iota(jnp.int32, (n, n), 1)

    def inside(first, several):
        keep = (c_at <= r_at) & (r_at % prompts == c_at % prompts)
        rows = [pl.ds(pl.multiple_of((first + u) * n, n), n) for u in range(several)]
        units = [(rows[u], i) for u in range(several) for i in range(groups)]
        cols = [slice(i * gk, (i + 1) * gk) for i in range(groups)]
        sums = [dot(mq_ref[...], halves(gs[at, cols[i]])) for at, i in units]
        near = []
        for (at, i), total in zip(units, sums):
            b, d0, d1 = total[:n], total[n : n + half], total[n + half :]
            q = qs[at, cols[i]].astype(f32)
            k = ks[at, cols[i]].astype(f32)
            sq[at, cols[i]] = (q * jnp.exp(b)).astype(bf16)
            near.append((
                (q[:half] * jnp.exp(d0)).astype(bf16),
                (k[:half] * jnp.exp(-d0)).astype(bf16),
                (q[half:] * jnp.exp(d1[half:])).astype(bf16),
                (k * jnp.exp(-d1)).astype(bf16),
            ))
        weights = []
        for (at, i), (q0, k0, q1, k1) in zip(units, near):
            for hh in range(group):
                hk = slice(hh * DK, (hh + 1) * DK)
                weights.append((at, i * group + hh, dot_nt(q0[:, hk], k0[:, hk]), dot_nt(q1[:, hk], k1[:, hk])))
        for at, h, w0, w1 in weights:
            hv = slice(h * DV, (h + 1) * DV)
            v = vs[at, hv]
            w0 = jnp.where(keep[:half, :half], w0, 0.0).astype(bf16)
            w1 = jnp.where(keep[half:], w1, 0.0).astype(bf16)
            oi[at, hv] = jnp.concatenate([dot(w0, v[:half]), dot(w1, v)], axis=0).astype(bf16)

    pairs = blocks // 2

    @pl.loop(0, pairs // 2)
    def _(pair):
        inside(2 * pair, 2)

    pass_on(groups - 1)

    @pl.loop(pairs // 2, pairs)
    def _(pair):
        inside(2 * pair, 2)

    def head_norm(block, h):
        factor = lax.rsqrt(jnp.mean(block * block, axis=-1, keepdims=True) + norm_eps)
        at = pl.ds(pl.multiple_of(me * vw + h * DV, DV), DV)
        return (block * factor * head_gain_ref[:, at]).astype(bf16)

    new = nd[...]
    q_d = (dot(new, wq[...]) * DK ** (-0.5)).astype(bf16).astype(f32)
    k_d = dot(new, wk[...]).astype(bf16).astype(f32)
    e_d = jnp.exp(decay_of(dot(new, wd[...]), 0))
    vrow_ref[...] = dot(new, wv[...]).astype(bf16).astype(f32)
    for h in range(heads):
        at = slice(h * DK, (h + 1) * DK)
        qet[h] = jnp.transpose(q_d[:, at] * e_d[:, at])
    for s, table in enumerate((e_d, k_d)):
        cols_ref[s] = jnp.transpose(jnp.concatenate([table[:, h * DK : (h + 1) * DK] for h in range(heads)], axis=0))
    attb[...] = jnp.zeros_like(attb)
    for h in range(heads):
        state_copy(h).wait()
        for s in range(seqs):
            row = (s // dec_own) * PAD + s % dec_own
            attb[row : row + 1, h * DV : (h + 1) * DV] = jnp.sum(
                sbuf[h % 2, s] * qet[h, :, row : row + 1], axis=0, keepdims=True
            )
        if h + 2 < heads:
            state_copy(h + 2).start()
    for h in range(heads):
        at, hv = slice(h * DK, (h + 1) * DK), slice(h * DV, (h + 1) * DV)
        score = jnp.sum(q_d[:, at] * k_d[:, at], axis=-1, keepdims=True)
        dl[:, hv] = head_norm(attb[:, hv] + score * vrow_ref[:, hv], h)
    my_cols = pl.ds(pl.multiple_of(me * vw, vw), vw)
    dec_keep = pltpu.make_async_copy(dl.at[mine], ndec_hbm.at[:, my_cols], d_local)
    dec_keep.start()
    dec_give = pltpu.make_async_remote_copy(
        src_ref=dl.at[theirs], dst_ref=ndec_hbm.at[:, my_cols], send_sem=d_send, recv_sem=d_recv,
        device_id={"tp": other}, device_id_type=MESH,
    )
    dec_give.start()

    def out_refs(side, j):
        rows = pl.ds(pl.multiple_of(side * own + j * n, n), n)
        return oi.at[rows], nrm_hbm.at[pl.ds(pl.multiple_of(j * n, n), n), my_cols]

    def keep_copy(j):
        src, dst = out_refs(me, j)
        return pltpu.make_async_copy(src, dst, out_local.at[j])

    def give_copy(j):
        src, dst = out_refs(other, j)
        return pltpu.make_async_remote_copy(
            src_ref=src, dst_ref=dst, send_sem=out_send.at[j], recv_sem=out_recv.at[j],
            device_id={"tp": other}, device_id_type=MESH,
        )

    for i in range(groups):
        for d in range(1, kv):
            incoming_copy(d, i).wait_recv()
    for h in range(heads):
        for p in range(prompts):
            st[h, p * DK : (p + 1) * DK, :] = sin[h * prompts + p].astype(f32)

    @pl.loop(0, blocks)
    def _(block):
        rows = pl.ds(pl.multiple_of(block * n, n), n)
        for h in range(heads):
            hk, hv = slice(h * DK, (h + 1) * DK), slice(h * DV, (h + 1) * DV)
            state = st[h]
            from_state = dot(each_prompt(sq[rows, hk], prompts), state.astype(bf16))
            oi[rows, hv] = head_norm(oi[rows, hv].astype(f32) + from_state, h)
            added = dot(turned(ek[rows, hk], prompts), vs[rows, hv])
            decay = jnp.transpose(jnp.exp(tots[block, :, hk]))
            for p in range(prompts):
                at = slice(p * DK, (p + 1) * DK)
                st[h, at, :] = state[at] * decay[:, p : p + 1] + added[at]
        side = block // (blocks // 2)
        j = block - side * (blocks // 2)

        @pl.when(side == me)
        def _():
            keep_copy(j).start()

        @pl.when(side != me)
        def _():
            give_copy(j).start()

    for d in range(1, kv):
        for h in range(heads):
            local_copy(d, h).wait_send()
        for i in range(groups):
            total_copy(d, i).wait_send()
            incoming_copy(d, i).wait_send()
    dec_keep.wait()
    dec_give.wait()

    @pl.loop(0, blocks // 2)
    def _(j):
        keep_copy(j).wait()
        give_copy(j).wait_send()
        give_copy(j).wait_recv()


def last_kernel(
    own_pos, prompts, heads, dec_own,
    nrm_hbm, ndec_hbm, w_hbm, ds_hbm, cols_hbm, vrow_hbm, ps_hbm,
    y_hbm, yd_hbm, po_hbm, do_hbm,
    nrm, w, yb, sb, yd, cols, vrow, ps,
    n_sem, w_sem, s_sem, y_sem, o_sem, a_sem,
):
    own = own_pos * prompts
    chunk = min(256, own)
    count = own // chunk
    pos = chunk // prompts
    width = w.shape[1]
    tile = width // heads
    seqs = 2 * dec_own

    def n_copy(j):
        at = pl.ds(j * chunk, chunk)
        return pltpu.make_async_copy(nrm_hbm.at[at], nrm.at[at], n_sem.at[j])

    def w_copy(t):
        at = pl.ds(t * tile, tile)
        return pltpu.make_async_copy(w_hbm.at[:, at], w.at[:, at], w_sem.at[t])

    def s_copy(h):
        return pltpu.make_async_copy(ds_hbm.at[:, h], sb.at[h], s_sem.at[h])

    def o_copy(h):
        return pltpu.make_async_copy(sb.at[h], do_hbm.at[:, h], o_sem.at[h])

    def y_copy(t):
        at = pl.ds(t * tile, tile)
        return pltpu.make_async_copy(yb.at[:, :, at], y_hbm.at[:, :, at], y_sem.at[t])

    first = w_hbm.shape[0] // 2
    w_first = [
        pltpu.make_async_copy(w_hbm.at[pl.ds(c * first, first), pl.ds(0, tile)], w.at[pl.ds(c * first, first), pl.ds(0, tile)], a_sem.at[c])
        for c in range(2)
    ]
    small = [
        pltpu.make_async_copy(src, dst, a_sem.at[2 + c])
        for c, (src, dst) in enumerate(((ndec_hbm, nrm.at[pl.ds(own, PAD)]), (cols_hbm, cols), (vrow_hbm, vrow), (ps_hbm, ps)))
    ]
    n_copy(0).start()
    for load in w_first + small:
        load.start()
    for j in range(1, count):
        n_copy(j).start()
    s_copy(0).start()
    ps_out = pltpu.make_async_copy(ps, po_hbm, a_sem.at[6])
    yd_out = pltpu.make_async_copy(yd, yd_hbm, a_sem.at[7])
    each = -(-seqs // count)
    for t in range(heads):
        at = slice(t * tile, (t + 1) * tile)
        if t == 0:
            n_copy(0).wait()
            for load in w_first:
                load.wait()
        else:
            w_copy(t).wait()
        if t + 1 < heads:
            w_copy(t + 1).start()
            s_copy(t + 1).start()
        for j in range(count):
            if t == 0 and j:
                n_copy(j).wait()
            if t == 0 and j == count - 1:
                small[0].wait()
            extra = PAD if j == count - 1 else 0
            block = dot(nrm[j * chunk : (j + 1) * chunk + extra, :], w[:, at])
            yb[j * pos : (j + 1) * pos, :, at] = block[:chunk].astype(bf16).reshape(pos, prompts, tile)
            if extra:
                yd[:, at] = block[chunk : chunk + dec_own].astype(bf16)
            if j == 0:
                s_copy(t).wait()
            if t == 0 and j == 0:
                for load in small[1:]:
                    load.wait()
                ps_out.start()
            for s in range(j * each, min(seqs, (j + 1) * each)):
                row = (s // dec_own) * PAD + s % dec_own
                v = vrow[row : row + 1, t * DV : (t + 1) * DV]
                at_row = slice(t * 2 * PAD + row, t * 2 * PAD + row + 1)
                sb[t, s] = sb[t, s] * cols[0, :, at_row] + cols[1, :, at_row] * v
        y_copy(t).start()
        o_copy(t).start()
    yd_out.start()
    for t in range(heads):
        y_copy(t).wait()
        o_copy(t).wait()
    ps_out.wait()
    yd_out.wait()


ANY = pl.BlockSpec(memory_space=pl.ANY)
VMEM = pl.BlockSpec(memory_space=pltpu.VMEM)
LIMIT = 62 * 1024 * 1024


def on_device(
    pieces, new_tokens, w_query, w_key, w_value, w_decay, decay_bias, norm_gain, head_gain, w_out, prompt_state, decode_state,
):
    kv = lax.axis_size("kv")
    qk = w_query.shape[1]
    heads = qk // DK
    vw = heads * DV
    own_pos, prompts, width = pieces.shape
    own = own_pos * prompts
    chunk = min(256, own)
    count = own // chunk
    rows = 2 * own
    blocks = rows // (STEP * prompts)
    dec_own = new_tokens.shape[0]
    seqs = 2 * dec_own
    part = DK // kv
    group = 2 if heads % 2 == 0 else 1
    groups = heads // group
    hp = heads * prompts
    mk, mq = (jnp.asarray(m, bf16) for m in sum_matrices(prompts))
    dma = pltpu.SemaphoreType.DMA
    nrm, ndec, prompt_out, cols, v_rows = pl.pallas_call(
        functools.partial(main_kernel, own_pos, prompts, heads, kv, dec_own),
        name="layer",
        out_shape=(
            jax.ShapeDtypeStruct((own, 2 * vw), bf16),
            jax.ShapeDtypeStruct((PAD, 2 * vw), bf16),
            jax.ShapeDtypeStruct(prompt_state.shape, f32),
            jax.ShapeDtypeStruct((2, DK, heads * 2 * PAD), f32),
            jax.ShapeDtypeStruct((2 * PAD, vw), f32),
        ),
        in_specs=[ANY, VMEM, ANY, ANY, ANY, ANY, VMEM, VMEM, VMEM, VMEM, VMEM, VMEM, ANY],
        out_specs=(ANY, ANY, VMEM, VMEM, VMEM),
        scratch_shapes=[
            pltpu.VMEM(pieces.shape, bf16),
            pltpu.VMEM((rows, width), bf16),
            pltpu.VMEM((2 * PAD, width), bf16),
            pltpu.VMEM((width, qk), bf16),
            pltpu.VMEM((width, qk), bf16),
            pltpu.VMEM((width, vw), bf16),
            pltpu.VMEM((width, qk), bf16),
            pltpu.VMEM((rows, qk), bf16),
            pltpu.VMEM((rows, qk), bf16),
            pltpu.VMEM((rows, vw), bf16),
            pltpu.VMEM((rows, qk), f32),
            pltpu.VMEM((rows, qk), bf16),
            pltpu.VMEM((rows, qk), bf16),
            pltpu.VMEM((rows, group * DK), bf16),
            pltpu.VMEM((rows, vw), bf16),
            pltpu.VMEM((blocks, 8, qk), f32),
            pltpu.VMEM((8, qk), f32),
            pltpu.VMEM((heads, prompts * DK, DV), f32),
            pltpu.VMEM((hp, DK, DV), bf16),
            pltpu.VMEM((kv, hp, part, DV), bf16),
            pltpu.VMEM((kv, hp, part, DV), bf16),
            pltpu.VMEM((hp, DK, DV), bf16),
            pltpu.VMEM((groups, 8, DK), f32),
            pltpu.VMEM((kv, groups, 8, DK), f32),
            pltpu.VMEM((kv, DK, 8), f32),
            pltpu.VMEM((2, seqs, DK, DV), f32),
            pltpu.VMEM((heads, DK, 2 * PAD), f32),
            pltpu.VMEM((2 * PAD, vw), f32),
            pltpu.VMEM((2 * PAD, vw), bf16),
            dma((count,)),
            dma((3 * groups + 1,)),
            dma((count,)),
            dma((count,)),
            dma,
            dma,
            dma((kv, heads)),
            dma((kv, heads)),
            dma((kv, groups)),
            dma((kv, groups)),
            dma((kv, groups)),
            dma((kv, groups)),
            dma((heads,)),
            dma((blocks // 2,)),
            dma((blocks // 2,)),
            dma((blocks // 2,)),
            dma,
            dma,
            dma,
        ],
        compiler_params=pltpu.CompilerParams(collective_id=0, has_side_effects=True, vmem_limit_bytes=LIMIT),
    )(
        pieces, new_tokens, w_query, w_key, w_value, w_decay, decay_bias[None], norm_gain[None], head_gain[None],
        mk, mq, prompt_state, decode_state,
    )
    return pl.pallas_call(
        functools.partial(last_kernel, own_pos, prompts, heads, dec_own),
        name="last",
        out_shape=(
            jax.ShapeDtypeStruct(pieces.shape, bf16),
            jax.ShapeDtypeStruct(new_tokens.shape, bf16),
            jax.ShapeDtypeStruct(prompt_state.shape, f32),
            jax.ShapeDtypeStruct(decode_state.shape, f32),
        ),
        in_specs=[ANY] * 7,
        out_specs=(ANY,) * 4,
        scratch_shapes=[
            pltpu.VMEM((own + PAD, 2 * vw), bf16),
            pltpu.VMEM(w_out.shape, bf16),
            pltpu.VMEM(pieces.shape, bf16),
            pltpu.VMEM((heads, seqs, DK, DV), f32),
            pltpu.VMEM(new_tokens.shape, bf16),
            pltpu.VMEM(cols.shape, f32),
            pltpu.VMEM(v_rows.shape, f32),
            pltpu.VMEM(prompt_state.shape, f32),
            dma((count,)),
            dma((heads,)),
            dma((heads,)),
            dma((heads,)),
            dma((heads,)),
            dma((8,)),
        ],
        compiler_params=pltpu.CompilerParams(vmem_limit_bytes=LIMIT),
    )(nrm, ndec, w_out, decode_state, cols, v_rows, prompt_out)


def solution(mesh):
    return jax.shard_map(
        on_device,
        mesh=mesh,
        in_specs=(
            P(("kv", "tp"), "dp", None),
            P(("dp", "kv", "tp"), None),
            P(None, "tp"),
            P(None, "tp"),
            P(None, "tp"),
            P(None, "tp"),
            P(),
            P(),
            P(),
            P(),
            P("dp", "tp", "kv", None),
            P(("dp", "kv"), "tp", None, None),
        ),
        out_specs=(
            P(("kv", "tp"), "dp", None),
            P(("dp", "kv", "tp"), None),
            P("dp", "tp", "kv", None),
            P(("dp", "kv"), "tp", None, None),
        ),
        check_vma=False,
    )
```

```python
import functools

import jax
import jax.numpy as jnp
import numpy as np
from jax import lax
from jax.experimental import pallas as pl
from jax.experimental.pallas import tpu as pltpu
from jax.sharding import PartitionSpec as P

DK = 128
DV = 256
STEP = 64
PART = 16

norm_eps = 0.1
decay_tau = 16.0
f32, bf16 = jnp.float32, jnp.bfloat16
MESH = pl.DeviceIdType.MESH
PAD = 16


def dot(a, b):
    return jnp.dot(a, b, preferred_element_type=f32)


def dot_nt(a, b):
    return lax.dot_general(a, b, (((1,), (1,)), ((), ())), preferred_element_type=f32)


def dot_tn(a, b):
    return lax.dot_general(a, b, (((0,), (0,)), ((), ())), preferred_element_type=f32)


def sum_matrices(prompts):
    n = STEP * prompts
    r, c = np.arange(n)[:, None], np.arange(n)[None]
    same = (r % prompts) == (c % prompts)

    def from_anchor(edge):
        return (same & (c >= edge) & (c <= r)) * 1.0 - (same & (c < edge) & (c > r)) * 1.0

    b = (same & (c <= r)) * 1.0
    rest = (same & (c > r)) * 1.0
    whole = ((np.arange(16)[:, None] == (c % prompts))) * 1.0
    d0 = from_anchor(PART * prompts)[: n // 2]
    d1 = from_anchor(3 * PART * prompts)
    for_keys = np.concatenate([rest, whole], axis=0)
    near = np.concatenate([b, d0, d1], axis=0)
    return np.concatenate([for_keys] * 2, axis=1), np.concatenate([near] * 2, axis=1)


def normed(rows, gain):
    wide = rows.astype(f32)
    factor = lax.rsqrt(jnp.mean(wide * wide, axis=-1, keepdims=True) + norm_eps)
    return wide * factor * gain


def halves(g):
    hi = g.astype(bf16)
    mid = (g - hi.astype(f32)).astype(bf16)
    return jnp.concatenate([hi, mid], axis=0)


def each_prompt(rows, prompts):
    row_prompt = lax.broadcasted_iota(jnp.int32, (rows.shape[0], 1), 0) % prompts
    zero = jnp.zeros_like(rows)
    return jnp.concatenate([jnp.where(row_prompt == p, rows, zero) for p in range(prompts)], axis=1)


def turned(rows, prompts):
    columns = jnp.transpose(rows)
    column_prompt = lax.broadcasted_iota(jnp.int32, (1, columns.shape[1]), 1) % prompts
    zero = jnp.zeros_like(columns)
    return jnp.concatenate([jnp.where(column_prompt == p, columns, zero) for p in range(prompts)], axis=0)


def by_prompt(table, row_prompt, prompts):
    picked = table[0:1]
    for p in range(1, prompts):
        picked = jnp.where(row_prompt == p, table[p : p + 1], picked)
    return picked


def main_kernel(
    own_pos, prompts, heads, kv, dec_own,
    x_hbm, dec_ref, wq_hbm, wk_hbm, wv_hbm, wd_hbm, bias_ref, gain_ref, head_gain_ref, mk_hbm, mq_hbm, ps_hbm, ds_hbm,
    nrm_hbm, ndec_hbm, po_ref, cols_ref, vrow_ref,
    xb, nb, nd, wq, wkd, wv, mk_ref, mq_ref, ps_ref, qs, ks, vs, gs, sq, ek, ew, oi, tots, later, st, loc, rx, inc, sin, tb, rxt, ttr,
    sbuf, qet, attb, scores, dl,
    x_sem, w_sem, n_send, n_recv, nd_send, nd_recv, p1_send, p1_recv, t_send, t_recv, p2_send, p2_recv,
    s_sem, out_local, out_send, out_recv, d_local, d_send, d_recv,
):
    me = lax.axis_index("tp")
    other = 1 - me
    here = lax.axis_index("kv")
    own = own_pos * prompts
    rows_all = 2 * own
    chunk = min(256, own)
    count = own // chunk
    n = STEP * prompts
    half = n // 2
    blocks = rows_all // n
    group = 2 if heads % 2 == 0 else 1
    groups = heads // group
    gk, gv = group * DK, group * DV
    near_group = 2 if heads % 2 == 0 else 1
    qk, vw = heads * DK, heads * DV
    part = DK // kv
    seqs = 2 * dec_own
    pos = chunk // prompts

    def x_copy(j):
        at = pl.ds(j * pos, pos)
        return pltpu.make_async_copy(x_hbm.at[at], xb.at[at], x_sem.at[j])

    for j in range(count):
        x_copy(j).start()
    loads = []
    for i in range(groups):
        kc, vc = pl.ds(i * gk, gk), pl.ds(i * gv, gv)
        for s, (src, dst) in enumerate((
            (wk_hbm.at[:, kc], wkd.at[:, pl.ds(2 * i * gk, gk)]),
            (wd_hbm.at[:, kc], wkd.at[:, pl.ds((2 * i + 1) * gk, gk)]),
            (wv_hbm.at[:, vc], wv.at[:, vc]),
        )):
            loads.append(pltpu.make_async_copy(src, dst, w_sem.at[3 * i + s]))
    for s, (src, dst) in enumerate(((wq_hbm, wq), (mk_hbm, mk_ref), (mq_hbm, mq_ref), (ps_hbm, ps_ref))):
        loads.append(pltpu.make_async_copy(src, dst, w_sem.at[3 * groups + s]))
    for load in loads:
        load.start()

    barrier = pltpu.get_barrier_semaphore()
    pl.semaphore_signal(barrier, inc=1, device_id={"tp": other}, device_id_type=MESH)
    for d in range(1, kv):
        pl.semaphore_signal(barrier, inc=1, device_id={"kv": lax.rem(here + d, kv)}, device_id_type=MESH)
    pl.semaphore_wait(barrier, kv)

    def state_copy(h):
        return pltpu.make_async_copy(ds_hbm.at[:, h], sbuf.at[lax.rem(h, 2)], s_sem.at[h])

    def piece_copy(j, side):
        rows = pl.ds(pl.multiple_of(side * own + j * chunk, chunk), chunk)
        return pltpu.make_async_remote_copy(
            src_ref=nb.at[rows], dst_ref=nb.at[rows], send_sem=n_send.at[j], recv_sem=n_recv.at[j],
            device_id={"tp": other}, device_id_type=MESH,
        )

    mine = pl.ds(pl.multiple_of(me * PAD, PAD), PAD)
    theirs = pl.ds(pl.multiple_of(other * PAD, PAD), PAD)
    dec_rows = normed(dec_ref[...], gain_ref[...])
    nd[mine, :] = jnp.concatenate([dec_rows, jnp.zeros((PAD - dec_own, dec_rows.shape[1]), f32)], axis=0).astype(bf16)
    dec_copy = pltpu.make_async_remote_copy(
        src_ref=nd.at[mine], dst_ref=nd.at[mine], send_sem=nd_send, recv_sem=nd_recv,
        device_id={"tp": other}, device_id_type=MESH,
    )
    small = min(32, pos)
    for j in range(count):
        x_copy(j).wait()

        @pl.loop(0, pos // small)
        def _(s):
            at = pl.multiple_of(j * pos + s * small, small)
            to = pl.ds(pl.multiple_of(me * own + at * prompts, small * prompts), small * prompts)
            nb[to, :] = xb[pl.ds(at, small)].reshape(small * prompts, xb.shape[2])
            nb[to, :] = normed(nb[to, :], gain_ref[...]).astype(bf16)

        if j == 0:
            dec_copy.start()
        else:
            piece_copy(j - 1, me).start()
    piece_copy(count - 1, me).start()

    def decay_of(product, i):
        at = pl.ds(pl.multiple_of(me * qk + i * gk, gk), product.shape[1])
        t = product + bias_ref[:, at]
        return (jnp.minimum(t, 0.0) - jnp.log1p(jnp.exp(-jnp.abs(t)))) * (1.0 / decay_tau)

    wide = min(512, own)

    def project(at, i):
        rows = pl.ds(pl.multiple_of(at, wide), wide)
        kc, vc = slice(i * gk, (i + 1) * gk), slice(i * gv, (i + 1) * gv)
        block = nb[rows, :]
        pair = dot(block, wkd[:, 2 * i * gk : 2 * (i + 1) * gk])
        ks[rows, kc] = pair[:, :gk].astype(bf16)
        gs[rows, kc] = decay_of(pair[:, gk:], i)
        vs[rows, vc] = dot(block, wv[:, vc]).astype(bf16)

    row_prompt = lax.broadcasted_iota(jnp.int32, (n, 1), 0) % prompts

    def at_odd(u):
        return u % 2 == 0

    def keys_of(i):
        kc = slice(i * gk, (i + 1) * gk)
        later[:, kc] = jnp.zeros((8, gk), f32)

        batch = 4 if blocks % 4 == 0 else 2

        @pl.loop(0, blocks // batch)
        def _(back):
            after = later[:, kc]
            places = [blocks - 1 - back * batch - u for u in range(batch)]
            spans = [pl.ds(pl.multiple_of(at * n, n), n) for at in places]
            together = [
                dot(mk_ref[...], jnp.concatenate([halves(gs[spans[u], kc]), halves(gs[spans[u + 1], kc])], axis=1))
                for u in range(0, batch, 2)
            ]
            for u in range(batch):
                at, rows = places[u], spans[u]
                sums = together[u // 2][:, (u % 2) * gk : (u % 2 + 1) * gk]
                end = ks[rows, kc].astype(f32) * jnp.exp(sums[:n])
                if at_odd(u):
                    ek[rows, kc] = end.astype(bf16)
                else:
                    ek[rows, kc] = (end * by_prompt(jnp.exp(following), row_prompt, prompts)).astype(bf16)
                    ew[pl.ds(pl.multiple_of((at // 2) * n, n), n), kc] = end.astype(bf16)
                sq[rows, :gk] = (end * by_prompt(jnp.exp(after), row_prompt, prompts)).astype(bf16)
                total = sums[n : n + 8]
                tots[at, :, kc] = total
                after, following = after + total, total
            later[:, kc] = after

        span = min(512, rows_all)
        for hh in range(group):
            st[i * group + hh] = jnp.zeros(st.shape[1:], f32)

        @pl.loop(0, rows_all // span)
        def _(c):
            rows = pl.ds(pl.multiple_of(c * span, span), span)
            for hh in range(group):
                h = i * group + hh
                st[h] = st[h] + dot(turned(sq[rows, hh * DK : (hh + 1) * DK], prompts), vs[rows, h * DV : (h + 1) * DV])

        for hh in range(group):
            h = i * group + hh
            for p in range(prompts):
                loc[h * prompts + p] = st[h, p * DK : (p + 1) * DK, :].astype(bf16)
                tb[i, hh * prompts + p : hh * prompts + p + 1, :] = later[p : p + 1, h * DK : (h + 1) * DK]
            for d in range(1, kv):
                local_copy(d, h).start()
        for d in range(1, kv):
            total_copy(d, i).start()

    def local_copy(d, h):
        to = lax.rem(here + d, kv)
        hp = pl.ds(h * prompts, prompts)
        return pltpu.make_async_remote_copy(
            src_ref=loc.at[hp, pl.ds(pl.multiple_of(to * part, part), part)], dst_ref=rx.at[d, hp],
            send_sem=p1_send.at[d, h], recv_sem=p1_recv.at[d, h], device_id={"kv": to}, device_id_type=MESH,
        )

    def total_copy(d, i):
        return pltpu.make_async_remote_copy(
            src_ref=tb.at[i], dst_ref=rxt.at[d, i], send_sem=t_send.at[d, i], recv_sem=t_recv.at[d, i],
            device_id={"kv": lax.rem(here + d, kv)}, device_id_type=MESH,
        )

    def incoming_copy(d, h):
        to = lax.rem(here + d, kv)
        hp = pl.ds(h * prompts, prompts)
        return pltpu.make_async_remote_copy(
            src_ref=inc.at[to, hp], dst_ref=sin.at[hp, pl.ds(pl.multiple_of(here * part, part), part)],
            send_sem=p2_send.at[d, h], recv_sem=p2_recv.at[d, h], device_id={"kv": to}, device_id_type=MESH,
        )

    my_part = pl.ds(pl.multiple_of(here * part, part), part)

    def pass_on(h):
        i, hh = h // group, h % group
        for d in range(1, kv):
            if hh == 0:
                total_copy(d, i).wait_recv()
            local_copy(d, h).wait_recv()
        if hh == 0:
            rxt[0, i] = tb[i]
            for c in range(kv):
                ttr[c] = jnp.transpose(jnp.exp(rxt[lax.rem(here - c + kv, kv), i]))
        for p in range(prompts):
            hp = h * prompts + p
            rx[0, hp] = loc[hp, my_part, :]
            running = ps_ref[p, h]
            at = hh * prompts + p
            for c in range(kv):
                inc[c, hp] = running.astype(bf16)
                running = running * ttr[c, my_part, at : at + 1] + rx[lax.rem(here - c + kv, kv), hp].astype(f32)
            po_ref[p, h] = running
        for d in range(1, kv):
            incoming_copy(d, h).start()
        for p in range(prompts):
            hp = h * prompts + p
            sin[hp, my_part, :] = inc[here, hp]

    for i in range(groups):
        for s in range(3):
            loads[3 * i + s].wait()
        if i == 0:
            @pl.loop(0, own // wide)
            def _(j):
                project(me * own + j * wide, 0)

            @pl.loop(0, own // wide)
            def _(j):
                for c in range(wide // chunk):
                    piece_copy(j * (wide // chunk) + c, other).wait_recv()
                project(other * own + j * wide, 0)

            for h in range(min(2, heads)):
                state_copy(h).start()
            for load in loads[3 * groups :]:
                load.wait()
        else:
            @pl.loop(0, rows_all // wide)
            def _(j):
                project(j * wide, i)

        if i:
            for hh in range(group):
                pass_on((i - 1) * group + hh)
        keys_of(i)


    for j in range(count):
        piece_copy(j, me).wait_send()
    dec_copy.wait()

    def head_norm(block, h):
        factor = lax.rsqrt(jnp.mean(block * block, axis=-1, keepdims=True) + norm_eps)
        at = pl.ds(pl.multiple_of(me * vw + h * DV, DV), DV)
        return (block * factor * head_gain_ref[:, at]).astype(bf16)

    new = nd[...]
    q_d = (dot(new, wq[...]) * DK ** (-0.5)).astype(bf16).astype(f32)
    pair_d = dot(new, wkd[...])
    k_d = jnp.concatenate([pair_d[:, 2 * i * gk : (2 * i + 1) * gk] for i in range(groups)], axis=1).astype(bf16).astype(f32)
    e_d = jnp.exp(jnp.concatenate([decay_of(pair_d[:, (2 * i + 1) * gk : 2 * (i + 1) * gk], i) for i in range(groups)], axis=1))
    vrow_ref[...] = dot(new, wv[...]).astype(bf16).astype(f32)
    for h in range(heads):
        at = slice(h * DK, (h + 1) * DK)
        qet[h] = jnp.transpose(q_d[:, at] * e_d[:, at])
        score = jnp.sum(q_d[:, at] * k_d[:, at], axis=-1, keepdims=True)
        scores[:, h * DV : (h + 1) * DV] = score * vrow_ref[:, h * DV : (h + 1) * DV]
    for s, table in enumerate((e_d, k_d)):
        cols_ref[s] = jnp.transpose(jnp.concatenate([table[:, h * DK : (h + 1) * DK] for h in range(heads)], axis=0))
    attb[...] = jnp.zeros_like(attb)

    def queries(j):
        rows = pl.ds(pl.multiple_of(j * wide, wide), wide)
        qs[rows, :] = (dot(nb[rows, :], wq[...]) * DK ** (-0.5)).astype(bf16)

    def attend(h):
        slot = lax.rem(h, 2)
        hv = pl.ds(pl.multiple_of(h * DV, DV), DV)
        for s in range(seqs):
            row = (s // dec_own) * PAD + s % dec_own
            attb[row : row + 1, hv] = jnp.sum(sbuf[slot, s] * qet[h, :, row : row + 1], axis=0, keepdims=True)

    @pl.loop(0, heads)
    def _(h):
        state_copy(h).wait()
        if rows_all // wide == heads:
            queries(h)
        attend(h)

        @pl.when(h + 2 < heads)
        def _():
            state_copy(h + 2).start()

    if rows_all // wide != heads:
        @pl.loop(0, rows_all // wide)
        def _(j):
            queries(j)

    for h in range(heads):
        hv = slice(h * DV, (h + 1) * DV)
        dl[:, hv] = head_norm(attb[:, hv] + scores[:, hv], h)
    my_cols = pl.ds(pl.multiple_of(me * vw, vw), vw)
    dec_keep = pltpu.make_async_copy(dl.at[mine], ndec_hbm.at[:, my_cols], d_local)
    dec_keep.start()
    dec_give = pltpu.make_async_remote_copy(
        src_ref=dl.at[theirs], dst_ref=ndec_hbm.at[:, my_cols], send_sem=d_send, recv_sem=d_recv,
        device_id={"tp": other}, device_id_type=MESH,
    )
    dec_give.start()

    r_at = lax.broadcasted_iota(jnp.int32, (n, n), 0)
    c_at = lax.broadcasted_iota(jnp.int32, (n, n), 1)

    def inside(pair):
        same = r_at % prompts == c_at % prompts
        keep = (c_at <= r_at) & same
        both = pl.ds(pl.multiple_of(pair * 2 * n, 2 * n), 2 * n)
        rows = [pl.ds(pl.multiple_of((2 * pair + u) * n, n), n) for u in range(2)]
        early = pl.ds(pl.multiple_of(pair * n, n), n)
        units = [(u, i) for u in range(2) for i in range(heads // near_group)]
        cols = [slice(i * near_group * DK, (i + 1) * near_group * DK) for i in range(heads // near_group)]
        sums = [dot(mq_ref[...], halves(gs[rows[u], cols[i]])) for u, i in units]
        near = []
        for (u, i), total in zip(units, sums):
            b, d0, d1 = total[:n], total[n : n + half], total[n + half :]
            q = qs[rows[u], cols[i]].astype(f32)
            k = ks[rows[u], cols[i]].astype(f32)
            start = q * jnp.exp(b)
            across = None
            if u:
                across = start.astype(bf16)
                start = start * by_prompt(jnp.exp(tots[2 * pair, :, cols[i]]), row_prompt, prompts)
            sq[rows[u], cols[i]] = start.astype(bf16)
            near.append((
                (q[:half] * jnp.exp(d0)).astype(bf16),
                (k[:half] * jnp.exp(-d0)).astype(bf16),
                (q[half:] * jnp.exp(d1[half:])).astype(bf16),
                (k * jnp.exp(-d1)).astype(bf16),
                across,
            ))
        weights = []
        for (u, i), (q0, k0, q1, k1, across) in zip(units, near):
            for hh in range(near_group):
                h = i * near_group + hh
                hk = slice(hh * DK, (hh + 1) * DK)
                w2 = dot_nt(across[:, hk], ew[early, h * DK : (h + 1) * DK]) if u else None
                weights.append((u, h, dot_nt(q0[:, hk], k0[:, hk]), dot_nt(q1[:, hk], k1[:, hk]), w2))
        for u, h, w0, w1, w2 in weights:
            hv = slice(h * DV, (h + 1) * DV)
            w0 = jnp.where(keep[:half, :half], w0, 0.0).astype(bf16)
            w1 = jnp.where(keep[half:], w1, 0.0).astype(bf16)
            v = vs[rows[0], hv]
            if u:
                v = vs[both, hv]
                w2 = jnp.where(same, w2, 0.0).astype(bf16)
                w0 = jnp.concatenate([w2[:half], w0], axis=1)
                w1 = jnp.concatenate([w2[half:], w1], axis=1)
            oi[rows[u], hv] = jnp.concatenate([dot(w0, v[: w0.shape[1]]), dot(w1, v)], axis=0).astype(bf16)

    pairs = blocks // 2

    due = [2 * pairs // 4 if hh == 0 else 3 * pairs // 4 for hh in range(group)]
    marks = sorted(set([0, pairs] + due))
    for low, high in zip(marks[:-1], marks[1:]):
        @pl.loop(low, high)
        def _(pair):
            inside(pair)

        for hh in range(group):
            if due[hh] == high:
                pass_on((groups - 1) * group + hh)

    def out_refs(side, j, i):
        rows = pl.ds(pl.multiple_of(side * own + j * 2 * n, 2 * n), 2 * n)
        to = pl.ds(pl.multiple_of(me * vw + i * gv, gv), gv)
        return oi.at[rows, pl.ds(i * gv, gv)], nrm_hbm.at[pl.ds(pl.multiple_of(j * 2 * n, 2 * n), 2 * n), to]

    def keep_copy(j, i):
        src, dst = out_refs(me, j, i)
        return pltpu.make_async_copy(src, dst, out_local.at[i, j])

    def give_copy(j, i):
        src, dst = out_refs(other, j, i)
        return pltpu.make_async_remote_copy(
            src_ref=src, dst_ref=dst, send_sem=out_send.at[i, j], recv_sem=out_recv.at[i, j],
            device_id={"tp": other}, device_id_type=MESH,
        )

    def scan(i):
        members = range(i * group, (i + 1) * group)
        for h in members:
            for d in range(1, kv):
                incoming_copy(d, h).wait_recv()
            for p in range(prompts):
                st[h, p * DK : (p + 1) * DK, :] = sin[h * prompts + p].astype(f32)

        @pl.loop(0, pairs)
        def _(pair):
            rows = pl.ds(pl.multiple_of(pair * 2 * n, 2 * n), 2 * n)
            for h in members:
                hk, hv = slice(h * DK, (h + 1) * DK), slice(h * DV, (h + 1) * DV)
                state = st[h]
                from_state = dot(each_prompt(sq[rows, hk], prompts), state.astype(bf16))
                oi[rows, hv] = head_norm(oi[rows, hv].astype(f32) + from_state, h)
                added = dot(turned(ek[rows, hk], prompts), vs[rows, hv])
                decay = jnp.transpose(jnp.exp(tots[2 * pair, :, hk] + tots[2 * pair + 1, :, hk]))
                for p in range(prompts):
                    at = slice(p * DK, (p + 1) * DK)
                    st[h, at, :] = state[at] * decay[:, p : p + 1] + added[at]
            side = pair // (pairs // 2)
            j = pair - side * (pairs // 2)

            @pl.when(side == me)
            def _():
                keep_copy(j, i).start()

            @pl.when(side != me)
            def _():
                give_copy(j, i).start()

    for i in range(groups):
        scan(i)

    for d in range(1, kv):
        for h in range(heads):
            local_copy(d, h).wait_send()
            incoming_copy(d, h).wait_send()
        for i in range(groups):
            total_copy(d, i).wait_send()
    dec_keep.wait()
    dec_give.wait()

    for i in range(groups):
        @pl.loop(0, pairs // 2)
        def _(j):
            keep_copy(j, i).wait()
            give_copy(j, i).wait_send()
            give_copy(j, i).wait_recv()


def last_kernel(
    own_pos, prompts, heads, dec_own,
    nrm_hbm, ndec_hbm, w_hbm, ds_hbm, cols_hbm, vrow_hbm, ps_hbm,
    y_hbm, yd_hbm, po_hbm, do_hbm,
    nrm, w, yb, sb, yd, cols, vrow, ps,
    n_sem, w_sem, s_sem, y_sem, o_sem, a_sem,
):
    own = own_pos * prompts
    chunk = min(512, own)
    count = own // chunk
    pos = chunk // prompts
    width = w.shape[1]
    tile = width // heads
    seqs = 2 * dec_own

    def n_copy(j):
        at = pl.ds(j * chunk, chunk)
        return pltpu.make_async_copy(nrm_hbm.at[at], nrm.at[at], n_sem.at[j])

    def w_copy(t):
        at = pl.ds(t * tile, tile)
        return pltpu.make_async_copy(w_hbm.at[:, at], w.at[:, at], w_sem.at[t])

    def s_copy(h):
        return pltpu.make_async_copy(ds_hbm.at[:, h], sb.at[h], s_sem.at[h])

    def o_copy(h):
        return pltpu.make_async_copy(sb.at[h], do_hbm.at[:, h], o_sem.at[h])

    def y_copy(t):
        at = pl.ds(t * tile, tile)
        return pltpu.make_async_copy(yb.at[:, :, at], y_hbm.at[:, :, at], y_sem.at[t])

    first = w_hbm.shape[0] // 2
    w_first = [
        pltpu.make_async_copy(w_hbm.at[pl.ds(c * first, first), pl.ds(0, tile)], w.at[pl.ds(c * first, first), pl.ds(0, tile)], a_sem.at[c])
        for c in range(2)
    ]
    small = [
        pltpu.make_async_copy(src, dst, a_sem.at[2 + c])
        for c, (src, dst) in enumerate(((ndec_hbm, nrm.at[pl.ds(own, PAD)]), (cols_hbm, cols), (vrow_hbm, vrow), (ps_hbm, ps)))
    ]
    n_copy(0).start()
    for load in w_first + small:
        load.start()
    for j in range(1, count):
        n_copy(j).start()
    s_copy(0).start()
    ps_out = pltpu.make_async_copy(ps, po_hbm, a_sem.at[6])
    yd_out = pltpu.make_async_copy(yd, yd_hbm, a_sem.at[7])
    each = -(-seqs // count)
    for t in range(heads):
        at = slice(t * tile, (t + 1) * tile)
        if t == 0:
            n_copy(0).wait()
            for load in w_first:
                load.wait()
        else:
            w_copy(t).wait()
        if t + 1 < heads:
            w_copy(t + 1).start()
            s_copy(t + 1).start()
        for j in range(count):
            if t == 0 and j:
                n_copy(j).wait()
            if t == 0 and j == count - 1:
                small[0].wait()
            extra = PAD if j == count - 1 else 0
            block = dot(nrm[j * chunk : (j + 1) * chunk + extra, :], w[:, at])
            yb[j * pos : (j + 1) * pos, :, at] = block[:chunk].astype(bf16).reshape(pos, prompts, tile)
            if extra:
                yd[:, at] = block[chunk : chunk + dec_own].astype(bf16)
            if j == 0:
                s_copy(t).wait()
            if t == 0 and j == 0:
                for load in small[1:]:
                    load.wait()
                ps_out.start()
            for s in range(j * each, min(seqs, (j + 1) * each)):
                row = (s // dec_own) * PAD + s % dec_own
                v = vrow[row : row + 1, t * DV : (t + 1) * DV]
                at_row = slice(t * 2 * PAD + row, t * 2 * PAD + row + 1)
                sb[t, s] = sb[t, s] * cols[0, :, at_row] + cols[1, :, at_row] * v
        y_copy(t).start()
        o_copy(t).start()
    yd_out.start()
    for t in range(heads):
        y_copy(t).wait()
        o_copy(t).wait()
    ps_out.wait()
    yd_out.wait()


ANY = pl.BlockSpec(memory_space=pl.ANY)
VMEM = pl.BlockSpec(memory_space=pltpu.VMEM)
LIMIT = 62 * 1024 * 1024


def on_device(
    pieces, new_tokens, w_query, w_key, w_value, w_decay, decay_bias, norm_gain, head_gain, w_out, prompt_state, decode_state,
):
    kv = lax.axis_size("kv")
    qk = w_query.shape[1]
    heads = qk // DK
    vw = heads * DV
    own_pos, prompts, width = pieces.shape
    own = own_pos * prompts
    chunk = min(256, own)
    count = own // chunk
    rows = 2 * own
    blocks = rows // (STEP * prompts)
    dec_own = new_tokens.shape[0]
    seqs = 2 * dec_own
    part = DK // kv
    group = 2 if heads % 2 == 0 else 1
    groups = heads // group
    hp = heads * prompts
    mk, mq = (jnp.asarray(m, bf16) for m in sum_matrices(prompts))
    dma = pltpu.SemaphoreType.DMA
    nrm, ndec, prompt_out, cols, v_rows = pl.pallas_call(
        functools.partial(main_kernel, own_pos, prompts, heads, kv, dec_own),
        name="layer",
        out_shape=(
            jax.ShapeDtypeStruct((own, 2 * vw), bf16),
            jax.ShapeDtypeStruct((PAD, 2 * vw), bf16),
            jax.ShapeDtypeStruct(prompt_state.shape, f32),
            jax.ShapeDtypeStruct((2, DK, heads * 2 * PAD), f32),
            jax.ShapeDtypeStruct((2 * PAD, vw), f32),
        ),
        in_specs=[ANY, VMEM, ANY, ANY, ANY, ANY, VMEM, VMEM, VMEM, ANY, ANY, ANY, ANY],
        out_specs=(ANY, ANY, VMEM, VMEM, VMEM),
        scratch_shapes=[
            pltpu.VMEM(pieces.shape, bf16),
            pltpu.VMEM((rows, width), bf16),
            pltpu.VMEM((2 * PAD, width), bf16),
            pltpu.VMEM((width, qk), bf16),
            pltpu.VMEM((width, 2 * qk), bf16),
            pltpu.VMEM((width, vw), bf16),
            pltpu.VMEM(mk.shape, bf16),
            pltpu.VMEM(mq.shape, bf16),
            pltpu.VMEM(prompt_state.shape, f32),
            pltpu.VMEM((rows, qk), bf16),
            pltpu.VMEM((rows, qk), bf16),
            pltpu.VMEM((rows, vw), bf16),
            pltpu.VMEM((rows, qk), f32),
            pltpu.VMEM((rows, qk), bf16),
            pltpu.VMEM((rows, qk), bf16),
            pltpu.VMEM((own, qk), bf16),
            pltpu.VMEM((rows, vw), bf16),
            pltpu.VMEM((blocks, 8, qk), f32),
            pltpu.VMEM((8, qk), f32),
            pltpu.VMEM((heads, prompts * DK, DV), f32),
            pltpu.VMEM((hp, DK, DV), bf16),
            pltpu.VMEM((kv, hp, part, DV), bf16),
            pltpu.VMEM((kv, hp, part, DV), bf16),
            pltpu.VMEM((hp, DK, DV), bf16),
            pltpu.VMEM((groups, 8, DK), f32),
            pltpu.VMEM((kv, groups, 8, DK), f32),
            pltpu.VMEM((kv, DK, 8), f32),
            pltpu.VMEM((2, seqs, DK, DV), f32),
            pltpu.VMEM((heads, DK, 2 * PAD), f32),
            pltpu.VMEM((2 * PAD, vw), f32),
            pltpu.VMEM((2 * PAD, vw), f32),
            pltpu.VMEM((2 * PAD, vw), bf16),
            dma((count,)),
            dma((3 * groups + 4,)),
            dma((count,)),
            dma((count,)),
            dma,
            dma,
            dma((kv, heads)),
            dma((kv, heads)),
            dma((kv, groups)),
            dma((kv, groups)),
            dma((kv, heads)),
            dma((kv, heads)),
            dma((heads,)),
            dma((groups, blocks // 4)),
            dma((groups, blocks // 4)),
            dma((groups, blocks // 4)),
            dma,
            dma,
            dma,
        ],
        compiler_params=pltpu.CompilerParams(collective_id=0, has_side_effects=True, vmem_limit_bytes=LIMIT),
    )(
        pieces, new_tokens, w_query, w_key, w_value, w_decay, decay_bias[None], norm_gain[None], head_gain[None],
        mk, mq, prompt_state, decode_state,
    )
    return pl.pallas_call(
        functools.partial(last_kernel, own_pos, prompts, heads, dec_own),
        name="last",
        out_shape=(
            jax.ShapeDtypeStruct(pieces.shape, bf16),
            jax.ShapeDtypeStruct(new_tokens.shape, bf16),
            jax.ShapeDtypeStruct(prompt_state.shape, f32),
            jax.ShapeDtypeStruct(decode_state.shape, f32),
        ),
        in_specs=[ANY] * 7,
        out_specs=(ANY,) * 4,
        scratch_shapes=[
            pltpu.VMEM((own + PAD, 2 * vw), bf16),
            pltpu.VMEM(w_out.shape, bf16),
            pltpu.VMEM(pieces.shape, bf16),
            pltpu.VMEM((heads, seqs, DK, DV), f32),
            pltpu.VMEM(new_tokens.shape, bf16),
            pltpu.VMEM(cols.shape, f32),
            pltpu.VMEM(v_rows.shape, f32),
            pltpu.VMEM(prompt_state.shape, f32),
            dma((own // min(512, own),)),
            dma((heads,)),
            dma((heads,)),
            dma((heads,)),
            dma((heads,)),
            dma((8,)),
        ],
        compiler_params=pltpu.CompilerParams(vmem_limit_bytes=LIMIT),
    )(nrm, ndec, w_out, decode_state, cols, v_rows, prompt_out)


def solution(mesh):
    return jax.shard_map(
        on_device,
        mesh=mesh,
        in_specs=(
            P(("kv", "tp"), "dp", None),
            P(("dp", "kv", "tp"), None),
            P(None, "tp"),
            P(None, "tp"),
            P(None, "tp"),
            P(None, "tp"),
            P(),
            P(),
            P(),
            P(),
            P("dp", "tp", "kv", None),
            P(("dp", "kv"), "tp", None, None),
        ),
        out_specs=(
            P(("kv", "tp"), "dp", None),
            P(("dp", "kv", "tp"), None),
            P("dp", "tp", "kv", None),
            P(("dp", "kv"), "tp", None, None),
        ),
        check_vma=False,
    )
```
